32 devices in a mesh: gr: 2 (over x), sp: 8 (over z, y), tp: 2 (over core).
Axes of the slice: x: 2, y: 2, z: 4, core: 2. Of those that a mesh axis runs over, the one named last changes fastest.
Arguments:
- tokens: bfloat16 [8, 1024, 4096], P('gr', 'sp'), parts along dimension 0, may hold values from -6 to 6
- key_weight: bfloat16 [4096, 2048], P('sp', 'tp'), may hold values from -0.09375 to 0.09375
- value_weight: bfloat16 [4096, 2048], P('sp', 'tp'), may hold values from -0.09375 to 0.09375
- log_decay: float32 [32, 8, 1024], P('tp', 'gr', 'sp'), parts along dimension 1, may hold values from -1 to 0, as said below
- new_query: bfloat16 [8, 2048], P('gr', 'tp'), parts along dimension 0, may hold values from -6 to 6
- new_key: bfloat16 [8, 2048], P('gr', 'tp'), parts along dimension 0, may hold values from -24 to 24
- new_value: bfloat16 [8, 2048], P('gr', 'tp'), parts along dimension 0, may hold values from -6 to 6
- step_decay: float32 [32, 8], P('tp', 'gr'), parts along dimension 1, may hold values from -1.5 to -0.05
- norm_gain: float32 [2048], P('tp'), may hold values from 0.1 to 1.9
Outputs:
- state_cache: float32 [512, 32, 64], P('gr', 'tp'), parts along dimension 0
- first_read: bfloat16 [8, 2048], P('gr', 'tp'), parts along dimension 0
The draws below stay inside these ranges and needn't reach their ends.
There are 2 independent parts, one for each index of `gr`. The reference program is written for one: setup_inputs(seed, part) draws one part's arguments, and reference() takes and returns one part's arrays. A program takes and returns all parts, laid end to end along the dimension named above; an argument that names none is the same for every part. Nothing has to cross between parts.
Inputs may be any that keep to these rules, and one draw needn't show every extreme that they name: `log_decay`: every entry is at most zero.
All inputs are finite; a program needn't handle non-finite values.
Results may differ from the reference program's by a relative error of at most 0.0053.
Values may be sent and summed in bfloat16 or wider, within the bound.
A program may use at most 64 MiB of HBM per device.

```python
import jax
import jax.numpy as jnp
from jax import lax

D = 4096
RETENTION_HEADS = 32
HEAD_DIM = 64
GROUP_PROMPTS = 4
SPAN = 128
PROMPT_LENGTH = 1024


def draw_log_decay(key, part):
    key_vectors = jax.random.split(jax.random.fold_in(key, 7), 7)
    fast_share = 0.5
    is_fast = jax.random.uniform(key_vectors[0], (RETENTION_HEADS,), jnp.float32) < fast_share
    fast_rate = jnp.exp(jax.random.uniform(key_vectors[1], (RETENTION_HEADS,), jnp.float32, jnp.log(1.0 / 60.0), jnp.log(1.0 / 30.0)))
    slow_rate = jax.random.uniform(key_vectors[2], (RETENTION_HEADS,), jnp.float32, 0.1, 0.5) * jnp.log(10.0) / PROMPT_LENGTH
    decay_speed = jnp.where(is_fast, fast_rate, slow_rate)
    blocks = PROMPT_LENGTH // SPAN
    block_multiplier = jnp.exp(jax.random.uniform(key_vectors[3], (GROUP_PROMPTS, blocks), jnp.float32, jnp.log(0.5), jnp.log(2.0)))
    block_multiplier = jnp.broadcast_to(block_multiplier[:, :, None], (GROUP_PROMPTS, blocks, SPAN)).reshape(GROUP_PROMPTS, PROMPT_LENGTH)
    approximate = jax.random.uniform(key_vectors[4], (RETENTION_HEADS, GROUP_PROMPTS, PROMPT_LENGTH), jnp.float32, 0.5, 1.5)
    surge_position = jax.random.uniform(key_vectors[5], (RETENTION_HEADS, GROUP_PROMPTS, PROMPT_LENGTH), jnp.float32) < 2.0 / PROMPT_LENGTH
    surge_length = jnp.log(jax.random.uniform(key_vectors[6], (RETENTION_HEADS, GROUP_PROMPTS, PROMPT_LENGTH), jnp.float32, 0.5, 0.8))
    decay_factor = -decay_speed[:, None, None] * block_multiplier[None, :, :] * approximate + jnp.where(surge_position, surge_length, 0.0)
    return decay_factor.astype(jnp.float32)


def shard_levels(rng, dims, shards, smallest, top_value):
    def one(dim, parts):
        draws = jax.random.uniform(jax.random.fold_in(jax.random.fold_in(rng, 6), dim), (parts,), jnp.float32, smallest / len(shards), top_value / len(shards))
        return jnp.repeat(jnp.exp(draws), dims[dim] // parts).reshape((-1,) + (1,) * (len(dims) - dim - 1))

    level = one(*shards[0])
    for cut in shards[1:]:
        level = level * one(*cut)
    return level


def normal_values(own_key, dims, deviation, limit, shards=(), held_as=jnp.bfloat16):
    drawn = deviation * jax.random.normal(own_key, dims, jnp.float32)
    if shards:
        drawn = drawn * shard_levels(own_key, dims, shards, -0.22, 0.18)
    return jnp.clip(drawn, -limit, limit).astype(held_as)


def setup_inputs(seed: int = 0, part: int = 0) -> dict:
    key_list = jax.random.split(jax.random.key(seed), 10)
    part_splits = jax.random.split(jax.random.fold_in(key_list[9], part), 10)
    return {
        "tokens": normal_values(part_splits[0], (GROUP_PROMPTS, PROMPT_LENGTH, D), 1.0, 6.0, ((1, 8),)),
        "key_weight": normal_values(key_list[1], (D, RETENTION_HEADS * HEAD_DIM), D ** -0.5, 0.09375, ((0, 8), (1, 2))),
        "value_weight": normal_values(key_list[2], (D, RETENTION_HEADS * HEAD_DIM), D ** -0.5, 0.09375, ((0, 8), (1, 2))),
        "log_decay": draw_log_decay(jax.random.fold_in(jax.random.fold_in(key_list[9], part), 71), part),
        "new_query": normal_values(part_splits[4], (GROUP_PROMPTS, RETENTION_HEADS * HEAD_DIM), 1.0, 6.0, ((1, 2),)),
        "new_key": normal_values(part_splits[5], (GROUP_PROMPTS, RETENTION_HEADS * HEAD_DIM), 4.0, 24.0, ((1, 2),)),
        "new_value": normal_values(part_splits[6], (GROUP_PROMPTS, RETENTION_HEADS * HEAD_DIM), 1.0, 6.0, ((1, 2),)),
        "step_decay": jnp.clip(-1.5 + 1.45 * jax.random.uniform(part_splits[7], (RETENTION_HEADS, GROUP_PROMPTS), jnp.float32) ** shard_levels(part_splits[7], (RETENTION_HEADS, GROUP_PROMPTS), ((0, 2),), -0.2, 0.2), -1.5, -0.05),
        "norm_gain": jnp.clip(1.0 + 0.18 * jax.random.normal(key_list[8], (RETENTION_HEADS * HEAD_DIM,), jnp.float32), 0.1, 1.9),
    }


def rotate_half(values, positions):
    half = values.shape[-1] // 2
    inverse = 10000.0 ** (-jnp.arange(half, dtype=jnp.float32) * (2.0 / values.shape[-1]))
    angles = positions[..., None] * inverse
    cosine = jnp.cos(angles)
    sine = jnp.sin(angles)
    first, second = (values[..., :half], values[..., half:])
    return jnp.concatenate([first * cosine - second * sine, second * cosine + first * sine], axis=-1)

def reference(tokens, key_weight, value_weight, log_decay, new_query, new_key, new_value, step_decay, norm_gain):
    seqs, length, width = tokens.shape
    heads = key_weight.shape[1] // HEAD_DIM
    token_rows = tokens.reshape(seqs * length, width)
    key_vectors = jnp.dot(token_rows, key_weight, preferred_element_type=jnp.float32).astype(jnp.bfloat16)
    values = jnp.dot(token_rows, value_weight, preferred_element_type=jnp.float32).astype(jnp.bfloat16)
    key_vectors = lax.optimization_barrier(key_vectors).astype(jnp.float32).reshape(seqs, length, heads, HEAD_DIM)
    values = lax.optimization_barrier(values).astype(jnp.float32).reshape(seqs, length, heads, HEAD_DIM)
    positions = jnp.arange(length, dtype=jnp.float32)
    rkeys = rotate_half(key_vectors, positions[None, :, None]) * HEAD_DIM ** (-0.5)
    totals = lax.optimization_barrier(jnp.sum(log_decay, axis=-1, keepdims=True))
    weight = jnp.exp(totals - jnp.cumsum(log_decay, axis=-1))
    weight_seq = jnp.transpose(weight, (1, 2, 0))

    def one_prompt(items):
        key_seq, value_seq, decay_seq = items
        weighted = key_seq * decay_seq[:, :, None]
        return jnp.einsum('tha,thb->hab', weighted, value_seq, precision=lax.Precision.HIGHEST)
    prompt_state = lax.map(one_prompt, (rkeys, values, weight_seq))
    end_pos = jnp.full((seqs, heads), float(length), jnp.float32)
    query = rotate_half(new_query.astype(jnp.float32).reshape(seqs, heads, HEAD_DIM), end_pos)
    key_new = rotate_half(new_key.astype(jnp.float32).reshape(seqs, heads, HEAD_DIM), end_pos) * HEAD_DIM ** (-0.5)
    value_new = new_value.astype(jnp.float32).reshape(seqs, heads, HEAD_DIM)
    state = jnp.exp(step_decay).T[:, :, None, None] * prompt_state + key_new[:, :, :, None] * value_new[:, :, None, :]
    raw = jnp.einsum('sha,shab->shb', query, state, precision=lax.Precision.HIGHEST)
    center = lax.optimization_barrier(jnp.mean(raw, axis=-1, keepdims=True))
    spread = lax.optimization_barrier(jnp.mean(jnp.square(raw - center), axis=-1, keepdims=True))
    normed = (raw - center) * lax.rsqrt(spread + 1e-06) * norm_gain.reshape(heads, HEAD_DIM)
    first_read = normed.reshape(seqs, heads * HEAD_DIM).astype(jnp.bfloat16)
    state_cache = jnp.transpose(state, (0, 2, 1, 3)).reshape(seqs * HEAD_DIM, heads, HEAD_DIM)
    return (state_cache, first_read)
```

```python
import functools

import jax
import jax.numpy as jnp
import numpy as np
from jax import lax
from jax.experimental import pallas as pl
from jax.experimental.pallas import tpu as pltpu
from jax.sharding import PartitionSpec as P

HEAD_DIM = 64
GROUPS = 2
MESH = pl.DeviceIdType.MESH
F32 = jnp.float32
HIGH = lax.Precision.HIGHEST


def kernel(
    sizes,
    tok, kw, vw, ld, cos_tab, sin_tab, nq, nk, nv, sd, gain,
    out, read,
    toks, w, lds, tots, wts, own_state, part, got, full, cos_ref, sin_ref, ends, qx, outer, decay, raw_ref,
    l_sem, w_sem, yw_s, yw_r, tok_s, tok_r, core_s, core_r, z_s, z_r, x_s, x_r,
    ld_s, ld_r, tot_s, tot_r, rs_s, rs_r, ag_s, ag_r, yg_s, yg_r,
):
    n_sp, seqs, span, heads = sizes
    n_a = n_sp // 2
    g, sp, tp = lax.axis_index("gr"), lax.axis_index("sp"), lax.axis_index("tp")
    a, b = sp // 2, sp % 2
    ob = 1 - b
    core = tp % 2
    mate = tp + 1 - 2 * core
    rows, width = tok.shape
    depth = kw.shape[0]
    cols = kw.shape[1] // 2
    n_c = cols // 128
    in_group = seqs // GROUPS
    group_rows = in_group * span
    group_state = in_group * HEAD_DIM
    hs = heads * seqs
    peer = a * 2 + ob
    y_peer = (g, peer, tp)
    x_peer = (1 - g, sp, tp)
    core_peer = (g, sp, mate)
    edge = jnp.logical_or(a == 0, a == n_a - 1)
    ahead = jnp.where(a < n_a // 2, 1, -1)

    def lanes(m):
        return pl.ds(m * 128 if isinstance(m, int) else pl.multiple_of(m * 128, 128), 128)

    def columns(side, j):
        return pl.ds(pl.multiple_of(side * cols + j * 128, 128), 128)

    def shard_rows(s):
        return pl.ds(pl.multiple_of(s * depth, depth), depth)

    def own_weight(m, j):
        return pltpu.make_async_copy(
            (kw, vw)[m].at[:, columns(b, j)], w.at[j, shard_rows(sp), lanes(m)], w_sem.at[m, j]
        )

    local = [
        pltpu.make_async_copy(ld, lds.at[b], l_sem.at[0]),
        pltpu.make_async_copy(tok, toks.at[b], l_sem.at[1]),
        pltpu.make_async_copy(cos_tab.at[pl.ds(pl.multiple_of(a * 2 * span, 8), 2 * span)], cos_ref, l_sem.at[2]),
        pltpu.make_async_copy(sin_tab.at[pl.ds(pl.multiple_of(a * 2 * span, 8), 2 * span)], sin_ref, l_sem.at[3]),
        pltpu.make_async_copy(cos_tab.at[pl.ds(n_sp * span, 8)], ends.at[0], l_sem.at[4]),
        pltpu.make_async_copy(sin_tab.at[pl.ds(n_sp * span, 8)], ends.at[1], l_sem.at[5]),
    ]
    for j in range(n_c):
        for m in range(2):
            own_weight(m, j).start()
    for c in local:
        c.start()

    barrier = pltpu.get_barrier_semaphore()

    @pl.loop(1, n_sp)
    def _(k):
        pl.semaphore_signal(barrier, inc=1, device_id=(g, lax.rem(sp + k, n_sp), tp), device_id_type=MESH)

    pl.semaphore_signal(barrier, inc=1, device_id=x_peer, device_id_type=MESH)
    pl.semaphore_signal(barrier, inc=1, device_id=core_peer, device_id_type=MESH)
    pl.semaphore_wait(barrier, n_sp + 1)

    def remote(src, dst, s, r, dev):
        return pltpu.make_async_remote_copy(
            src_ref=src, dst_ref=dst, send_sem=s, recv_sem=r, device_id=dev, device_id_type=MESH
        )

    def yw(m, j):
        return remote(
            (kw, vw)[m].at[:, columns(ob, j)], w.at[j, shard_rows(sp), lanes(m)], yw_s.at[m, j], yw_r.at[m, j], y_peer
        )

    def half_group(h):
        half = group_rows // 2
        return pl.ds(pl.multiple_of(h * group_rows + core * half, half), half)

    def ytok(h):
        return remote(tok.at[half_group(h)], toks.at[b, half_group(h)], tok_s.at[h], tok_r.at[h], y_peer)

    def ytok_in(h):
        here = toks.at[ob, half_group(h)]
        return remote(here, here, tok_s.at[h], tok_r.at[h], y_peer)

    def ctok(h):
        here = toks.at[ob, half_group(h)]
        return remote(here, here, core_s.at[h], core_r.at[h], core_peer)

    yld = remote(ld, lds.at[b], ld_s, ld_r, y_peer)

    early = min(2, n_c)
    soon = min(3, n_c)
    for m in range(2):
        @pl.when(g == m)
        def _():
            for j in range(early):
                yw(m, j).start()
            yld.start()
            for j in range(early):
                yw(1 - m, j).start()
            for j in range(early, soon):
                yw(m, j).start()
            ytok(0).start()
            for j in range(soon, n_c):
                yw(m, j).start()
            for j in range(early, n_c):
                yw(1 - m, j).start()
            for h in range(1, GROUPS):
                ytok(h).start()

    def yw_wait(m_is_g, j):
        for m in range(2):
            @pl.when(g == (m if m_is_g else 1 - m))
            def _():
                yw(m, j).wait_recv()

    def zsend(j, s, t):
        ref = w.at[j, shard_rows(s), lanes(g)]
        return remote(ref, ref, z_s.at[(t + 1) // 2, j, s], z_r.at[j, s], (g, sp + 2 * t, tp))

    def xsend(j, s):
        ref = w.at[j, shard_rows(s), lanes(g)]
        return remote(ref, ref, x_s.at[j, s], x_r.at[j, s], x_peer)

    def xrecv(j, s):
        ref = w.at[j, shard_rows(s), lanes(1 - g)]
        return remote(ref, ref, x_s.at[j, s], x_r.at[j, s], x_peer)

    def exists(place):
        return jnp.logical_and(place >= 0, place < n_a)

    def launch(j, s):
        for t in (-ahead, ahead):
            @pl.when(exists(a + t))
            def _():
                zsend(j, s, t).start()

    def start_chunk(j):
        own_weight(0, j).wait()
        own_weight(1, j).wait()
        launch(j, sp)
        yw_wait(True, j)
        launch(j, peer)

    def zstep(j, d, bb):
        side = b if bb == 0 else ob
        for t in (ahead, -ahead):
            @pl.when(exists(a + t * d))
            def _():
                s = (a + t * d) * 2 + side
                zsend(j, s, -t).wait_recv()

                @pl.when(exists(a - t))
                def _():
                    zsend(j, s, -t).start()

                xsend(j, s).start()

    def gather_x(j):
        yw_wait(False, j)

        @pl.loop(0, n_sp)
        def _(s):
            @pl.when(s // 2 != a)
            def _():
                xrecv(j, s).wait_recv()

    start_chunk(0)

    def tsend(k):
        return remote(tots.at[sp], tots.at[sp], tot_s.at[k], tot_r.at[k], (g, lax.rem(sp + k, n_sp), tp))

    for c in local:
        c.wait()
    raw_ref[...] = jnp.zeros(raw_ref.shape, F32)
    tots[sp] = jnp.zeros(tots.shape[1:], F32)
    tots[sp, :, 0:hs] = lax.dot_general(
        jnp.ones((8, span), F32), lds[b], (((1,), (1,)), ((), ())), precision=HIGH, preferred_element_type=F32
    )

    lanes_at = lax.broadcasted_iota(jnp.int32, (HEAD_DIM, 128), 1)
    subs_at = lax.broadcasted_iota(jnp.int32, (HEAD_DIM, 128), 0)
    diagonal = lanes_at % HEAD_DIM == subs_at
    same_head = jnp.where(
        lax.broadcasted_iota(jnp.int32, (128, 128), 0) // HEAD_DIM
        == lax.broadcasted_iota(jnp.int32, (128, 128), 1) // HEAD_DIM, 1.0, 0.0
    ).astype(F32)

    def exact(x, y):
        return jnp.dot(x, y, precision=HIGH, preferred_element_type=F32)

    def at_end(u):
        low = lax.broadcasted_iota(jnp.int32, u.shape, 1) % HEAD_DIM < HEAD_DIM // 2
        turned = jnp.where(low, pltpu.roll(u, 128 - 32, 1), pltpu.roll(u, 32, 1))
        return u * ends[0, 0:1, :] + turned * ends[1, 0:1, :]

    head_lane = lax.broadcasted_iota(jnp.int32, (heads, 2 * cols), 1) // HEAD_DIM
    head_row = lax.broadcasted_iota(jnp.int32, (heads, 2 * cols), 0)
    spread_heads = jnp.where(head_lane == head_row, 1.0, 0.0).astype(F32)
    decay[...] = jnp.exp(exact(sd[...], spread_heads))

    @pl.loop(1, n_sp)
    def _(k):
        tsend(k).start()

    def new_token(c0):
        chunk = pl.ds(c0, 128)
        query = at_end(nq[:, chunk].astype(F32)) * HEAD_DIM ** 0.5
        key_new = at_end(nk[:, chunk].astype(F32))
        value_new = nv[:, chunk].astype(F32)
        for s in range(seqs):
            at = pl.ds(s * HEAD_DIM, HEAD_DIM)
            qx[at, chunk] = exact(jnp.where(diagonal, query[s:s + 1], 0.0), same_head)
            column = exact(jnp.where(diagonal, key_new[s:s + 1], 0.0), same_head)
            outer[at, chunk] = column * value_new[s:s + 1]

    def weigh():
        yld.wait_recv()

        @pl.loop(1, n_sp)
        def _(k):
            tsend(k).wait_recv()

        pos_t = lax.broadcasted_iota(jnp.int32, (span, span), 0)
        pos_u = lax.broadcasted_iota(jnp.int32, (span, span), 1)
        later_mask = jnp.where(pos_u > pos_t, 1.0, 0.0).astype(F32)
        row_hs = lax.broadcasted_iota(jnp.int32, (hs, cols), 0)
        lane_head = lax.broadcasted_iota(jnp.int32, (hs, cols), 1) // HEAD_DIM + b * (heads // 2)
        for tb in range(2):
            inside = lax.dot_general(
                later_mask, lds[tb], (((1,), (1,)), ((), ())), precision=HIGH, preferred_element_type=F32
            )
            index = a * 2 + tb

            def add(k, total):
                return total + jnp.where(k > index, tots[k], 0.0)

            after = lax.fori_loop(0, n_sp, add, jnp.zeros(tots.shape[1:], F32))
            suffix = inside + after[0:1, :hs]
            for s in range(seqs):
                select = jnp.where(row_hs == lane_head * seqs + s, 1.0, 0.0).astype(F32)
                wts[tb, s] = jnp.exp(jnp.dot(suffix, select, precision=HIGH, preferred_element_type=F32))

    lane = lax.broadcasted_iota(jnp.int32, (span, 128), 1)
    first = lane % HEAD_DIM < HEAD_DIM // 2
    lane_out = lax.broadcasted_iota(jnp.int32, (HEAD_DIM, 128), 1)

    def states(tb, h, j):
        at = pl.ds(pl.multiple_of(h * group_rows, group_rows), group_rows)
        prod = jnp.dot(toks[tb, at, :], w[j], preferred_element_type=F32)
        keys = prod[:, :128].astype(jnp.bfloat16).astype(F32)
        values = prod[:, 128:].astype(jnp.bfloat16)
        spot = pl.ds(pl.multiple_of(tb * span, span), span)
        result = []
        for i in range(in_group):
            u = keys[i * span:(i + 1) * span]
            turned = jnp.where(first, pltpu.roll(u, 128 - 32, 1), pltpu.roll(u, 32, 1))
            rk = u * cos_ref[spot, :] + turned * sin_ref[spot, :]
            weighted = (rk * wts[tb, h * in_group + i, :, pl.ds(j * 128, 128)]).astype(jnp.bfloat16)
            term = lax.dot_general(
                weighted, values[i * span:(i + 1) * span], (((0,), (0,)), ((), ())), preferred_element_type=F32
            )
            result.append(jnp.where(lane_out < HEAD_DIM, term[:HEAD_DIM], term[HEAD_DIM:]))
        return jnp.concatenate(result, axis=0)

    def own(j):
        @pl.loop(0, GROUPS)
        def _(h):
            own_state[h, j] = states(b, h, j)

    def reducer(h):
        return n_a // 2 - 1 + h

    def rs(h, j):
        to = reducer(h)
        return remote(part.at[h, j], got.at[a, j], rs_s.at[h, j], rs_r.at[a, j], (g, to * 2 + b, tp))

    def rs_in(src, h, j):
        return remote(part.at[h, j], got.at[src, j], rs_s.at[h, j], rs_r.at[src, j], y_peer)

    def partner(h, j):
        part[h, j] = (own_state[h, j] + states(ob, h, j)).astype(jnp.bfloat16)

        @pl.when(a != reducer(h))
        def _():
            rs(h, j).start()

    def ag(h, j, to):
        here = full.at[b, h, j]
        return remote(here, here, ag_s.at[j, to], ag_r.at[h, j], (g, to * 2 + b, tp))

    def yg(h, j, side):
        here = full.at[side, h, j]
        return remote(here, here, yg_s.at[h, j], yg_r.at[h, j], y_peer)

    def reduce(h, j):
        @pl.when(a == reducer(h))
        def _():
            def add(k, total):
                src = lax.rem(a + k, n_a)
                rs_in(src, h, j).wait_recv()
                return total + got[src, j].astype(F32)

            total = lax.fori_loop(1, n_a, add, part[h, j].astype(F32))
            full[b, h, j] = total.astype(jnp.bfloat16)

            @pl.loop(1, n_a)
            def _(k):
                ag(h, j, lax.rem(a + k, n_a)).start()

            yg(h, j, b).start()

    def collect(h, j):
        @pl.when(a != reducer(h))
        def _():
            ag(h, j, a).wait_recv()
            yg(h, j, b).start()

    def finish(side, h, j):
        chunk = columns(side, j)
        raws, done = [], []
        for i in range(in_group):
            s = h * in_group + i
            at = pl.ds(s * HEAD_DIM, HEAD_DIM)
            summed = full[side, h, j, i * HEAD_DIM:(i + 1) * HEAD_DIM, :].astype(F32)
            state = decay[s:s + 1, chunk] * summed + outer[at, chunk]
            raws.append(jnp.sum(qx[at, chunk] * state, axis=0, keepdims=True))
            done.append(state)
        out[chunk, h * group_state:(h + 1) * group_state] = jnp.concatenate(done, axis=0).T
        raw_ref[side * n_c + j, h * in_group:(h + 1) * in_group, :] = jnp.concatenate(raws, axis=0)

    def tokens_in(h):
        ytok_in(h).wait_recv()
        ctok(h).start()

    new_chunks = list(range(0, 2 * cols, 128))
    last = n_c - 1
    for j in range(n_c):
        if j > 0:
            @pl.when(jnp.logical_not(edge))
            def _():
                start_chunk(j)

        for step in range(6):
            zstep(j, step // 2 + 1, step % 2)
            if step == 2 and j < last:
                @pl.when(edge)
                def _():
                    start_chunk(j + 1)
            if j == 0:
                for c0 in new_chunks[step::4] if step < 4 else ():
                    new_token(c0)
                if step == 3:
                    weigh()
            else:
                if step == 2:
                    gather_x(j - 1)
                    own(j - 1)
                if j == last - 1 and step == 3:
                    tokens_in(0)
                if j == last - 1 and step == 4:
                    ctok(0).wait_recv()
                    for k in range(last - 1):
                        partner(0, k)
                if j == last and step == 3:
                    if last < 2:
                        tokens_in(0)
                        ctok(0).wait_recv()
                    partner(0, last - 1)
                if j == last and step == 4:
                    for k in range(last - 1):
                        reduce(0, k)
                if j == last and step == 5:
                    for k in range(last - 1):
                        collect(0, k)

        @pl.loop(4, n_a)
        def _(d):
            for bb in range(2):
                zstep(j, d, bb)

    tokens_in(1)
    reduce(0, last - 1)
    ctok(1).wait_recv()
    for j in range(last):
        partner(1, j)
    collect(0, last - 1)
    gather_x(last)
    own(last)
    for h in range(GROUPS):
        partner(h, last)
    for j in range(last):
        reduce(1, j)
    for j in range(last):
        collect(1, j)
    for h in range(GROUPS):
        reduce(h, last)
    for j in range(last):
        finish(b, 0, j)
        yg(0, j, ob).wait_recv()
        finish(ob, 0, j)
    for j in range(last):
        finish(b, 1, j)
        yg(1, j, ob).wait_recv()
        finish(ob, 1, j)
    for h in range(GROUPS):
        collect(h, last)
    for h in range(GROUPS):
        finish(b, h, last)
    for h in range(GROUPS):
        yg(h, last, ob).wait_recv()
        finish(ob, h, last)

    count = 2 * n_c
    raw = jnp.concatenate([raw_ref[c] for c in range(count)], axis=0)
    off = raw - exact(raw, same_head) * (1.0 / HEAD_DIM)
    spread = exact(off * off, same_head) * (1.0 / HEAD_DIM)
    normed = off * lax.rsqrt(spread + 1e-06)
    for c in range(count):
        chunk = pl.ds(c * 128, 128)
        read[:, chunk] = (normed[c * 8:c * 8 + seqs] * gain[:, chunk]).astype(jnp.bfloat16)

    for h in range(GROUPS):
        for j in range(n_c):
            yg(h, j, b).wait_send()

            @pl.when(a != reducer(h))
            def _():
                rs(h, j).wait_send()

            @pl.when(a == reducer(h))
            def _():
                @pl.loop(1, n_a)
                def _(k):
                    ag(h, j, lax.rem(a + k, n_a)).wait_send()

        ytok(h).wait_send()
        ctok(h).wait_send()

    @pl.loop(1, n_sp)
    def _(k):
        tsend(k).wait_send()

    yld.wait_send()
    for j in range(n_c):
        for m in range(2):
            yw(m, j).wait_send()
        for s in (sp, peer):
            for t in (-ahead, ahead):
                @pl.when(exists(a + t))
                def _():
                    zsend(j, s, t).wait_send()

    @pl.loop(0, n_c)
    def _(j):
        @pl.loop(1, n_a)
        def _(d):
            for side in (b, ob):
                for t in (ahead, -ahead):
                    @pl.when(exists(a + t * d))
                    def _():
                        s = (a + t * d) * 2 + side

                        @pl.when(exists(a - t))
                        def _():
                            zsend(j, s, -t).wait_send()

                        xsend(j, s).wait_send()


def prompt_states(token_rows, key_weight, value_weight, decays, cos, sin, step, seqs, span, heads, n_sp):
    rows, width = token_rows.shape
    depth, whole = key_weight.shape
    cols = whole // 2
    n_c = cols // 128
    n_a = n_sp // 2
    hs = heads * seqs
    state_rows = seqs * HEAD_DIM
    group_state = state_rows // GROUPS
    dma = pltpu.SemaphoreType.DMA
    bf16 = jnp.bfloat16
    hbm = pl.BlockSpec(memory_space=pl.ANY)
    vmem = pl.BlockSpec(memory_space=pltpu.VMEM)
    operands = (token_rows, key_weight, value_weight, decays, cos, sin, *step)
    return pl.pallas_call(
        functools.partial(kernel, (n_sp, seqs, span, heads)),
        out_shape=(
            pltpu.VMEM((whole, state_rows), F32),
            pltpu.VMEM((seqs, whole), bf16),
        ),
        in_specs=[hbm] * 6 + [vmem] * 5,
        out_specs=(vmem, vmem),
        scratch_shapes=[
            pltpu.VMEM((2, rows, width), bf16),
            pltpu.VMEM((n_c, n_sp * depth, 256), bf16),
            pltpu.VMEM((2, hs, span), F32),
            pltpu.VMEM((n_sp, 8, 128), F32),
            pltpu.VMEM((2, seqs, span, cols), F32),
            pltpu.VMEM((GROUPS, n_c, group_state, 128), F32),
            pltpu.VMEM((GROUPS, n_c, group_state, 128), bf16),
            pltpu.VMEM((n_a, n_c, group_state, 128), bf16),
            pltpu.VMEM((2, GROUPS, n_c, group_state, 128), bf16),
            pltpu.VMEM((2 * span, 128), F32),
            pltpu.VMEM((2 * span, 128), F32),
            pltpu.VMEM((2, 8, 128), F32),
            pltpu.VMEM((state_rows, whole), F32),
            pltpu.VMEM((state_rows, whole), F32),
            pltpu.VMEM((seqs, whole), F32),
            pltpu.VMEM((2 * n_c, 8, 128), F32),
            dma((6,)), dma((2, n_c)), dma((2, n_c)), dma((2, n_c)),
            dma((GROUPS,)), dma((GROUPS,)), dma((GROUPS,)), dma((GROUPS,)),
            dma((2, n_c, n_sp)), dma((n_c, n_sp)), dma((n_c, n_sp)), dma((n_c, n_sp)),
            dma, dma, dma((n_sp,)), dma((n_sp,)),
            dma((GROUPS, n_c)), dma((n_a, n_c)), dma((n_c, n_a)), dma((GROUPS, n_c)),
            dma((GROUPS, n_c)), dma((GROUPS, n_c)),
        ],
        compiler_params=pltpu.CompilerParams(
            collective_id=0, has_side_effects=True, vmem_limit_bytes=40 * 1024 * 1024
        ),
    )(*[pltpu.with_memory_space_constraint(v, pltpu.HBM) for v in operands])


def position_tables(length):
    half = HEAD_DIM // 2
    inverse = np.float32(10000.0) ** (-np.arange(half, dtype=np.float32) * np.float32(2.0 / HEAD_DIM))
    angles = np.arange(length + 8, dtype=np.float32)[:, None] * inverse[None, :].astype(np.float32)
    cosine = np.cos(angles.astype(np.float64)) * HEAD_DIM ** -0.5
    sine = np.sin(angles.astype(np.float64)) * HEAD_DIM ** -0.5
    cos = np.concatenate([cosine] * 4, axis=-1).astype(np.float32)
    sin = np.concatenate([-sine, sine] * 2, axis=-1).astype(np.float32)
    return cos, sin


def shards(
    tokens, key_weight, value_weight, log_decay, new_query, new_key, new_value, step_decay, norm_gain
):
    seqs, span, width = tokens.shape
    heads = key_weight.shape[1] // HEAD_DIM
    n_sp = lax.axis_size("sp")
    token_rows = tokens.reshape(seqs * span, width)
    decays = log_decay.reshape(heads * seqs, span)
    cos, sin = position_tables(span * n_sp)
    step = (new_query, new_key, new_value, step_decay.T, norm_gain.reshape(1, -1))
    state, read = prompt_states(
        token_rows, key_weight, value_weight, decays, jnp.asarray(cos), jnp.asarray(sin), step,
        seqs, span, heads, n_sp,
    )
    return (state.T.reshape(seqs * HEAD_DIM, heads, HEAD_DIM), read)


def solution(mesh):
    placed = (
        P("gr", "sp", None),
        P("sp", "tp"),
        P("sp", "tp"),
        P("tp", "gr", "sp"),
        P("gr", "tp"),
        P("gr", "tp"),
        P("gr", "tp"),
        P("tp", "gr"),
        P("tp"),
    )
    return jax.shard_map(
        shards,
        mesh=mesh,
        in_specs=placed,
        out_specs=(P("gr", "tp", None), P("gr", "tp")),
        check_vma=False,
    )
```

```python
import functools

import jax
import jax.numpy as jnp
import numpy as np
from jax import lax
from jax.experimental import pallas as pl
from jax.experimental.pallas import tpu as pltpu
from jax.sharding import PartitionSpec as P

HEAD_DIM = 64
PAIR = 2
MESH = pl.DeviceIdType.MESH
F32 = jnp.float32
HIGH = lax.Precision.HIGHEST


def kernel(
    sizes,
    tok, kw, vw, ld, cos_tab, sin_tab, nq, nk, nv, sd, gain,
    out, read,
    staged, read_at, toks, w, lds, tots, wts, own_state, part, got, full, cos_ref, sin_ref, ends, qx, outer, decay, raw_ref, acc,
    l_sem, w_sem, yw_s, yw_r, tok_s, tok_r, core_s, core_r, z_s, z_r, x_s, x_r,
    ld_s, ld_r, tot_s, tot_r, rs_s, rs_r, ag_s, ag_r, yg_s, yg_r, ac_s, out_sem,
):
    n_sp, seqs, span, heads = sizes
    n_a = n_sp // 2
    g, sp, tp = lax.axis_index("gr"), lax.axis_index("sp"), lax.axis_index("tp")
    a, b = sp // 2, sp % 2
    ob = 1 - b
    core = tp % 2
    mate = tp + 1 - 2 * core
    rows, width = tok.shape
    depth = kw.shape[0]
    cols = kw.shape[1] // 2
    n_c = cols // 128
    last = n_c - 1
    pair_rows = PAIR * span
    pair_state = PAIR * HEAD_DIM
    hs = heads * seqs
    peer = a * 2 + ob
    y_peer = (g, peer, tp)
    x_peer = (1 - g, sp, tp)
    core_peer = (g, sp, mate)
    edge = jnp.logical_or(a == 0, a == n_a - 1)
    ahead = jnp.where(a < n_a // 2, 1, -1)

    def lanes(m):
        return pl.ds(m * 128 if isinstance(m, int) else pl.multiple_of(m * 128, 128), 128)

    def columns(side, j):
        return pl.ds(pl.multiple_of(side * cols + j * 128, 128), 128)

    def shard_rows(s):
        return pl.ds(pl.multiple_of(s * depth, depth), depth)

    def own_weight(m, j):
        return pltpu.make_async_copy(
            (kw, vw)[m].at[:, columns(b, j)], w.at[j, shard_rows(sp), lanes(m)], w_sem.at[j]
        )

    local = [
        pltpu.make_async_copy(ld, lds.at[b], l_sem.at[0]),
        pltpu.make_async_copy(tok, toks.at[b], l_sem.at[1]),
        pltpu.make_async_copy(cos_tab.at[pl.ds(pl.multiple_of(a * 2 * span, 8), 2 * span)], cos_ref, l_sem.at[2]),
        pltpu.make_async_copy(sin_tab.at[pl.ds(pl.multiple_of(a * 2 * span, 8), 2 * span)], sin_ref, l_sem.at[3]),
        pltpu.make_async_copy(cos_tab.at[pl.ds(n_sp * span, 8)], ends.at[0], l_sem.at[4]),
        pltpu.make_async_copy(sin_tab.at[pl.ds(n_sp * span, 8)], ends.at[1], l_sem.at[5]),
    ]
    for j in range(n_c):
        for m in range(2):
            own_weight(m, j).start()
    for c in local:
        c.start()

    barrier = pltpu.get_barrier_semaphore()

    @pl.loop(1, n_sp)
    def _(k):
        pl.semaphore_signal(barrier, inc=1, device_id=(g, lax.rem(sp + k, n_sp), tp), device_id_type=MESH)

    pl.semaphore_signal(barrier, inc=1, device_id=x_peer, device_id_type=MESH)
    pl.semaphore_signal(barrier, inc=1, device_id=core_peer, device_id_type=MESH)
    pl.semaphore_wait(barrier, n_sp + 1)

    def remote(src, dst, s, r, dev):
        return pltpu.make_async_remote_copy(
            src_ref=src, dst_ref=dst, send_sem=s, recv_sem=r, device_id=dev, device_id_type=MESH
        )

    def drain(ref, sem):
        pltpu.make_async_copy(ref, ref, sem).wait()

    def yw(m, j):
        return remote(
            (kw, vw)[m].at[:, columns(ob, j)], w.at[j, shard_rows(sp), lanes(m)], yw_s, yw_r.at[m, j], y_peer
        )

    def half_prompt(s):
        half = span // 2
        return pl.ds(pl.multiple_of(s * span + core * half, half), half)

    def ytok(h):
        return remote(tok.at[half_prompt(h)], toks.at[b, half_prompt(h)], tok_s, tok_r.at[h], y_peer)

    def ytok_in(h):
        here = toks.at[ob, half_prompt(h)]
        return remote(here, here, tok_s, tok_r.at[h], y_peer)

    def ctok(h):
        here = toks.at[ob, half_prompt(h)]
        return remote(here, here, core_s, core_r.at[h], core_peer)

    yld = remote(ld, lds.at[b], ld_s, ld_r, y_peer)

    early = min(2, n_c)
    soon = min(3, n_c)
    for m in range(2):
        @pl.when(g == m)
        def _():
            for j in range(early):
                yw(m, j).start()
            yld.start()
            for j in range(early):
                yw(1 - m, j).start()
            for j in range(early, soon):
                yw(m, j).start()
            for h in range(seqs // 2):
                ytok(h).start()
            for j in range(soon, n_c):
                yw(m, j).start()
            for j in range(early, last):
                yw(1 - m, j).start()
            for h in range(seqs // 2, seqs):
                ytok(h).start()
            for j in range(max(early, last), n_c):
                yw(1 - m, j).start()

    def yw_wait(m_is_g, j):
        for m in range(2):
            @pl.when(g == (m if m_is_g else 1 - m))
            def _():
                yw(m, j).wait_recv()

    def zsend(j, s, t):
        ref = w.at[j, shard_rows(s), lanes(g)]
        return remote(ref, ref, z_s.at[(t + 1) // 2], z_r.at[j, s], (g, sp + 2 * t, tp))

    def xsend(j, s):
        ref = w.at[j, shard_rows(s), lanes(g)]
        return remote(ref, ref, x_s, x_r.at[j if j < last else last + s // 2], x_peer)

    def exists(place):
        return jnp.logical_and(place >= 0, place < n_a)

    def launch(j, s):
        for t in (-ahead, ahead):
            @pl.when(exists(a + t))
            def _():
                zsend(j, s, t).start()

    def start_own(j):
        drain(w.at[j, shard_rows(sp)], w_sem.at[j])
        launch(j, sp)

    def start_chunk(j):
        if j >= early:
            start_own(j)
        yw_wait(True, j)
        launch(j, peer)

    def zstep(j, d, bb):
        side = b if bb == 0 else ob
        for t in (ahead, -ahead):
            @pl.when(exists(a + t * d))
            def _():
                s = (a + t * d) * 2 + side
                zsend(j, s, -t).wait_recv()

                @pl.when(exists(a - t))
                def _():
                    zsend(j, s, -t).start()

                xsend(j, s).start()

    def gather_x(j):
        yw_wait(False, j)
        drain(w.at[j, pl.ds(0, 2 * (n_a - 1) * depth), lanes(0)], x_r.at[j])

    for j in range(early):
        start_own(j)
    start_chunk(0)

    def tsend(k):
        return remote(tots.at[a], tots.at[a], tot_s, tot_r.at[k], (g, lax.rem(a + k, n_a) * 2 + b, tp))

    for c in local:
        c.wait()
    raw_ref[...] = jnp.zeros(raw_ref.shape, F32)
    tots[a] = jnp.zeros(tots.shape[1:], F32)

    def shard_total(tb):
        return lax.dot_general(
            jnp.ones((8, span), F32), lds[tb], (((1,), (1,)), ((), ())), precision=HIGH, preferred_element_type=F32
        )

    def total():
        yld.wait_recv()
        tots[a, :, 0:hs] = shard_total(0) + shard_total(1)

        @pl.loop(1, n_a)
        def _(k):
            tsend(k).start()

    lanes_at = lax.broadcasted_iota(jnp.int32, (HEAD_DIM, 128), 1)
    subs_at = lax.broadcasted_iota(jnp.int32, (HEAD_DIM, 128), 0)
    diagonal = lanes_at % HEAD_DIM == subs_at
    same_head = jnp.where(
        lax.broadcasted_iota(jnp.int32, (128, 128), 0) // HEAD_DIM
        == lax.broadcasted_iota(jnp.int32, (128, 128), 1) // HEAD_DIM, 1.0, 0.0
    ).astype(F32)

    def exact(x, y):
        return jnp.dot(x, y, precision=HIGH, preferred_element_type=F32)

    def at_end(u):
        low = lax.broadcasted_iota(jnp.int32, u.shape, 1) % HEAD_DIM < HEAD_DIM // 2
        turned = jnp.where(low, pltpu.roll(u, 128 - 32, 1), pltpu.roll(u, 32, 1))
        return u * ends[0, 0:1, :] + turned * ends[1, 0:1, :]

    head_lane = lax.broadcasted_iota(jnp.int32, (heads, 2 * cols), 1) // HEAD_DIM
    head_row = lax.broadcasted_iota(jnp.int32, (heads, 2 * cols), 0)
    spread_heads = jnp.where(head_lane == head_row, 1.0, 0.0).astype(F32)
    decay[...] = jnp.exp(exact(sd[...], spread_heads))

    def new_token(c0):
        chunk = pl.ds(c0, 128)
        query = at_end(nq[:, chunk].astype(F32)) * HEAD_DIM ** 0.5
        key_new = at_end(nk[:, chunk].astype(F32))
        value_new = nv[:, chunk].astype(F32)
        for s in range(seqs):
            at = pl.ds(s * HEAD_DIM, HEAD_DIM)
            qx[at, chunk] = exact(jnp.where(diagonal, query[s:s + 1], 0.0), same_head)
            column = exact(jnp.where(diagonal, key_new[s:s + 1], 0.0), same_head)
            outer[at, chunk] = column * value_new[s:s + 1]

    def weigh():
        @pl.loop(1, n_a)
        def _(k):
            tsend(k).wait_recv()

        pos_t = lax.broadcasted_iota(jnp.int32, (span, span), 0)
        pos_u = lax.broadcasted_iota(jnp.int32, (span, span), 1)
        later_mask = jnp.where(pos_u > pos_t, 1.0, 0.0).astype(F32)
        row_hs = lax.broadcasted_iota(jnp.int32, (hs, cols), 0)
        lane_head = lax.broadcasted_iota(jnp.int32, (hs, cols), 1) // HEAD_DIM + b * (heads // 2)

        def add(k, total):
            return total + jnp.where(k > a, tots[k], 0.0)

        after = lax.fori_loop(0, n_a, add, jnp.zeros(tots.shape[1:], F32))
        for tb in range(2):
            inside = lax.dot_general(
                later_mask, lds[tb], (((1,), (1,)), ((), ())), precision=HIGH, preferred_element_type=F32
            )
            suffix = inside + after[0:1, :hs]
            if tb == 0:
                suffix = suffix + shard_total(1)[0:1]
            for s in range(seqs):
                select = jnp.where(row_hs == lane_head * seqs + s, 1.0, 0.0).astype(F32)
                wts[tb, s] = jnp.exp(jnp.dot(suffix, select, precision=HIGH, preferred_element_type=F32))

    lane = lax.broadcasted_iota(jnp.int32, (span, 128), 1)
    first = lane % HEAD_DIM < HEAD_DIM // 2
    lane_out = lax.broadcasted_iota(jnp.int32, (HEAD_DIM, 128), 1)

    def states(tb, s, n, j):
        at = pl.ds(pl.multiple_of(s * span, span), n * span)
        return contract(jnp.dot(toks[tb, at, :], w[j], preferred_element_type=F32), tb, s, n, j)

    def contract(prod, tb, s, n, j):
        keys = prod[:, :128].astype(jnp.bfloat16).astype(F32)
        values = prod[:, 128:].astype(jnp.bfloat16)
        spot = pl.ds(pl.multiple_of(tb * span, span), span)
        result = []
        for i in range(n):
            u = keys[i * span:(i + 1) * span]
            turned = jnp.where(first, pltpu.roll(u, 128 - 32, 1), pltpu.roll(u, 32, 1))
            rk = u * cos_ref[spot, :] + turned * sin_ref[spot, :]
            weighted = (rk * wts[tb, s + i, :, pl.ds(j * 128, 128)]).astype(jnp.bfloat16)
            term = lax.dot_general(
                weighted, values[i * span:(i + 1) * span], (((0,), (0,)), ((), ())), preferred_element_type=F32
            )
            result.append(jnp.where(lane_out < HEAD_DIM, term[:HEAD_DIM], term[HEAD_DIM:]))
        return result

    def accumulate(place, fresh=False):
        rows_at = pl.ds(pl.multiple_of(place * 2 * depth, 2 * depth), 2 * depth)
        for k, tb in enumerate((b, ob)):
            for r in range(0, rows, pair_rows):
                new = jnp.dot(
                    toks[tb, r:r + pair_rows, rows_at], w[last, rows_at, :], preferred_element_type=F32
                )
                acc[k, r:r + pair_rows] = new if fresh else acc[k, r:r + pair_rows] + new

    def take(d):
        for t in (ahead, -ahead):
            @pl.when(exists(a + t * d))
            def _():
                drain(w.at[last, pl.ds(0, 2 * depth), lanes(0)], x_r.at[last + a + t * d])
                accumulate(a + t * d)

    def own(j):
        @pl.loop(0, seqs // PAIR)
        def _(p):
            for i, state in enumerate(states(b, p * PAIR, PAIR, j)):
                own_state[p * PAIR + i, j] = state

    def reducer(s):
        return n_a // 2 - 1 + s % 2

    def rs(s, j):
        to = reducer(s)
        return remote(part.at[s, j], got.at[a, s // 2, j], rs_s.at[s % 2], rs_r.at[s // 2, j], (g, to * 2 + b, tp))

    def partner(s, n, j):
        for i, state in enumerate(states(ob, s, n, j)):
            part[s + i, j] = (own_state[s + i, j] + state).astype(jnp.bfloat16)
        for i in range(n):
            rs_start(s + i, j)

    def rs_start(s, j):
        @pl.when(a != reducer(s))
        def _():
            rs(s, j).start()

    def ag(s, j, to):
        here = full.at[b, s, j]
        return remote(here, here, ag_s, ag_r.at[s, j], (g, to * 2 + b, tp))

    def direct(s, j):
        return s == seqs - 1 or j == last

    def across(s, j, to):
        here = full.at[b, s, j]
        return remote(here, here, ac_s.at[0 if j == last else 1], yg_r.at[s, j], (g, to * 2 + ob, tp))

    def yg(s, j, side):
        here = full.at[side, s, j]
        return remote(here, here, yg_s, yg_r.at[s, j], y_peer)

    def reduce(s, j):
        @pl.when(a == reducer(s))
        def _():
            drain(got.at[pl.ds(0, n_a - 1), s // 2, j], rs_r.at[s // 2, j])

            def add(k, total):
                return total + got[lax.rem(a + k, n_a), s // 2, j].astype(F32)

            total = lax.fori_loop(1, n_a, add, part[s, j].astype(F32))
            full[b, s, j] = total.astype(jnp.bfloat16)

            @pl.loop(1, n_a)
            def _(k):
                to = lax.rem(a + k, n_a)
                if direct(s, j):
                    across(s, j, to).start()
                ag(s, j, to).start()

            if direct(s, j):
                across(s, j, a).start()
            else:
                yg(s, j, b).start()

    def collect(s, j):
        @pl.when(a != reducer(s))
        def _():
            ag(s, j, a).wait_recv()
            if not direct(s, j):
                yg(s, j, b).start()

    def finish(side, p, j):
        chunk = columns(side, j)
        raws, done = [], []
        for i in range(PAIR):
            s = p * PAIR + i
            at = pl.ds(s * HEAD_DIM, HEAD_DIM)
            state = decay[s:s + 1, chunk] * full[side, s, j].astype(F32) + outer[at, chunk]
            raws.append(jnp.sum(qx[at, chunk] * state, axis=0, keepdims=True))
            done.append(state)
        staged[chunk, p * pair_state:(p + 1) * pair_state] = jnp.concatenate(done, axis=0).T
        raw_ref[side * n_c + j, p * PAIR:(p + 1) * PAIR, :] = jnp.concatenate(raws, axis=0)

    def put(side, j):
        return pltpu.make_async_copy(staged.at[columns(side, j)], out.at[columns(side, j)], out_sem)

    def tokens_in(s):
        ytok_in(s).wait_recv()
        ctok(s).start()

    def normalize(chunks):
        if not chunks:
            return
        raw = jnp.concatenate([raw_ref[c] for c in chunks], axis=0)
        off = raw - exact(raw, same_head) * (1.0 / HEAD_DIM)
        spread = exact(off * off, same_head) * (1.0 / HEAD_DIM)
        normed = off * lax.rsqrt(spread + 1e-06)
        for i, c in enumerate(chunks):
            chunk = pl.ds(c * 128, 128)
            read_at[:, chunk] = (normed[i * 8:i * 8 + seqs] * gain[:, chunk]).astype(jnp.bfloat16)

    new_chunks = list(range(0, 2 * cols, 128))
    for j in range(n_c):
        if j > 0:
            @pl.when(jnp.logical_not(edge))
            def _():
                start_chunk(j)

        for step in range(6):
            zstep(j, step // 2 + 1, step % 2)
            if step == 2 and j < last:
                @pl.when(edge)
                def _():
                    start_chunk(j + 1)
            if j == 0:
                for c0 in new_chunks[step::4] if step < 4 else ():
                    new_token(c0)
                if step == 3:
                    total()
            else:
                if j == 1 and step == 1:
                    weigh()
                if step == 2:
                    gather_x(j - 1)
                    own(j - 1)
                if j == last - 1 and step == 3:
                    for s in range(seqs // 2):
                        tokens_in(s)
                if j == last - 1 and step == 4:
                    for s in range(seqs // 2):
                        ctok(s).wait_recv()
                    for k in range(last - 1):
                        partner(0, PAIR, k)
                if j == last and step == 3:
                    if last < 2:
                        for s in range(seqs // 2):
                            tokens_in(s)
                            ctok(s).wait_recv()
                    for s in range(seqs // 2, seqs - 1):
                        tokens_in(s)
                    partner(0, PAIR, last - 1)
                    for s in range(seqs // 2, seqs - 1):
                        ctok(s).wait_recv()
                        for k in range(last):
                            partner(s, 1, k)
                if j == last and step == 4:
                    tokens_in(seqs - 1)
                    for s in range(seqs // 2):
                        for k in range(last - 1):
                            reduce(s, k)
                if j == last and step == 5:
                    ctok(seqs - 1).wait_recv()
                    for k in range(last):
                        partner(seqs - 1, 1, k)

        @pl.loop(4, n_a)
        def _(d):
            for bb in range(2):
                zstep(j, d, bb)

    if last == 0:
        weigh()
        for s in range(seqs):
            tokens_in(s)
        for s in range(seqs):
            ctok(s).wait_recv()
    yw_wait(False, last)
    accumulate(a, True)
    take(1)
    for s in range(seqs // 2):
        for k in range(max(last - 1, 0), last):
            reduce(s, k)
    for s in range(seqs // 2, seqs - 1):
        for k in range(last):
            reduce(s, k)
    take(2)
    for s in range(seqs // 2):
        for k in range(last - 1):
            collect(s, k)
    take(3)

    @pl.loop(4, n_a)
    def _(d):
        take(d)

    sums = [contract(acc[0], b, 0, seqs, last), contract(acc[1], ob, 0, seqs, last)]
    for s in range(seqs):
        part[s, last] = (sums[0][s] + sums[1][s]).astype(jnp.bfloat16)
    for s in range(seqs):
        rs_start(s, last)
    for k in range(last):
        reduce(seqs - 1, k)
    for s in range(seqs // 2):
        for k in range(max(last - 1, 0), last):
            collect(s, k)
    for s in range(seqs // 2, seqs - 1):
        for k in range(last):
            collect(s, k)
    for s in range(seqs):
        reduce(s, last)
    for j in range(last):
        for s in range(PAIR):
            yg(s, j, ob).wait_recv()
        finish(b, 0, j)
        finish(ob, 0, j)
    for j in range(last):
        for p in range(1, seqs // PAIR):
            for s in range(p * PAIR, (p + 1) * PAIR):
                if direct(s, j):
                    collect(s, j)
                yg(s, j, ob).wait_recv()
            finish(b, p, j)
            finish(ob, p, j)
        put(b, j).start()
        put(ob, j).start()
    normalize([side * n_c + j for side in range(2) for j in range(last)])
    for s in range(seqs):
        collect(s, last)
        yg(s, last, ob).wait_recv()
    for side in (b, ob):
        for p in range(seqs // PAIR):
            finish(side, p, last)
        put(side, last).start()
    normalize([side * n_c + last for side in range(2)])
    read_out = pltpu.make_async_copy(read_at, read, l_sem.at[0])
    read_out.start()

    for parity in range(2):
        @pl.when(a != reducer(parity))
        def _():
            drain(part.at[pl.ds(0, seqs // 2)], rs_s.at[parity])

        @pl.when(a == reducer(parity))
        def _():
            drain(got.at[pl.ds(0, n_a - 1)], ag_s)
            drain(got.at[:, :, 0], ac_s.at[0])
            if parity == (seqs - 1) % 2 and last > 0:
                drain(got.at[:, 0, pl.ds(0, last)], ac_s.at[1])

    if last > 0:
        drain(full.at[0, pl.ds(0, seqs - 1), pl.ds(0, last)], yg_s)
    drain(toks.at[0, pl.ds(0, rows // 2)], tok_s)
    drain(toks.at[0, pl.ds(0, rows // 2)], core_s)
    drain(tots.at[pl.ds(0, n_a - 1)], tot_s)
    yld.wait_send()
    drain(w.at[:, pl.ds(0, depth)], yw_s)
    drain(w.at[:, pl.ds(0, 2 * (n_a - 1) * depth), lanes(0)], x_s)
    for k in range(n_a):
        @pl.when(a == k)
        def _():
            if k < n_a - 1:
                drain(w.at[:, pl.ds(0, 2 * (k + 1) * depth), lanes(0)], z_s.at[1])
            if k > 0:
                drain(w.at[:, pl.ds(0, 2 * (n_a - k) * depth), lanes(0)], z_s.at[0])

    drain(staged, out_sem)
    read_out.wait()


def prompt_states(token_rows, key_weight, value_weight, decays, cos, sin, step, seqs, span, heads, n_sp):
    rows, width = token_rows.shape
    depth, whole = key_weight.shape
    cols = whole // 2
    n_c = cols // 128
    last = n_c - 1
    n_a = n_sp // 2
    hs = heads * seqs
    state_rows = seqs * HEAD_DIM
    dma = pltpu.SemaphoreType.DMA
    bf16 = jnp.bfloat16
    hbm = pl.BlockSpec(memory_space=pl.ANY)
    vmem = pl.BlockSpec(memory_space=pltpu.VMEM)
    operands = (token_rows, key_weight, value_weight, decays, cos, sin, *step)
    return pl.pallas_call(
        functools.partial(kernel, (n_sp, seqs, span, heads)),
        out_shape=(
            pltpu.VMEM((whole, state_rows), F32),
            pltpu.VMEM((seqs, whole), bf16),
        ),
        in_specs=[hbm] * 6 + [vmem] * 5,
        out_specs=(hbm, hbm),
        scratch_shapes=[
            pltpu.VMEM((whole, state_rows), F32),
            pltpu.VMEM((seqs, whole), bf16),
            pltpu.VMEM((2, rows, width), bf16),
            pltpu.VMEM((n_c, n_sp * depth, 256), bf16),
            pltpu.VMEM((2, hs, span), F32),
            pltpu.VMEM((n_a, 8, 128), F32),
            pltpu.VMEM((2, seqs, span, cols), F32),
            pltpu.VMEM((seqs, n_c, HEAD_DIM, 128), F32),
            pltpu.VMEM((seqs, n_c, HEAD_DIM, 128), bf16),
            pltpu.VMEM((n_a, seqs // 2, n_c, HEAD_DIM, 128), bf16),
            pltpu.VMEM((2, seqs, n_c, HEAD_DIM, 128), bf16),
            pltpu.VMEM((2 * span, 128), F32),
            pltpu.VMEM((2 * span, 128), F32),
            pltpu.VMEM((2, 8, 128), F32),
            pltpu.VMEM((state_rows, whole), F32),
            pltpu.VMEM((state_rows, whole), F32),
            pltpu.VMEM((seqs, whole), F32),
            pltpu.VMEM((2 * n_c, 8, 128), F32),
            pltpu.VMEM((2, rows, 256), F32),
            dma((6,)), dma((n_c,)), dma, dma((2, n_c)),
            dma, dma((seqs,)), dma, dma((seqs,)),
            dma((2,)), dma((n_c, n_sp)), dma, dma((last + n_a,)),
            dma, dma, dma, dma((n_a,)),
            dma((2,)), dma((seqs // 2, n_c)), dma, dma((seqs, n_c)),
            dma, dma((seqs, n_c)), dma((2,)), dma,
        ],
        compiler_params=pltpu.CompilerParams(
            collective_id=0, has_side_effects=True, vmem_limit_bytes=40 * 1024 * 1024
        ),
    )(*[pltpu.with_memory_space_constraint(v, pltpu.HBM) for v in operands])


def position_tables(length):
    half = HEAD_DIM // 2
    inverse = np.float32(10000.0) ** (-np.arange(half, dtype=np.float32) * np.float32(2.0 / HEAD_DIM))
    angles = np.arange(length + 8, dtype=np.float32)[:, None] * inverse[None, :].astype(np.float32)
    cosine = np.cos(angles.astype(np.float64)) * HEAD_DIM ** -0.5
    sine = np.sin(angles.astype(np.float64)) * HEAD_DIM ** -0.5
    cos = np.concatenate([cosine] * 4, axis=-1).astype(np.float32)
    sin = np.concatenate([-sine, sine] * 2, axis=-1).astype(np.float32)
    return cos, sin


def shards(
    tokens, key_weight, value_weight, log_decay, new_query, new_key, new_value, step_decay, norm_gain
):
    seqs, span, width = tokens.shape
    heads = key_weight.shape[1] // HEAD_DIM
    n_sp = lax.axis_size("sp")
    token_rows = tokens.reshape(seqs * span, width)
    decays = log_decay.reshape(heads * seqs, span)
    cos, sin = position_tables(span * n_sp)
    step = (new_query, new_key, new_value, step_decay.T, norm_gain.reshape(1, -1))
    state, read = prompt_states(
        token_rows, key_weight, value_weight, decays, jnp.asarray(cos), jnp.asarray(sin), step,
        seqs, span, heads, n_sp,
    )
    return (state.T.reshape(seqs * HEAD_DIM, heads, HEAD_DIM), read)


def solution(mesh):
    placed = (
        P("gr", "sp", None),
        P("sp", "tp"),
        P("sp", "tp"),
        P("tp", "gr", "sp"),
        P("gr", "tp"),
        P("gr", "tp"),
        P("gr", "tp"),
        P("tp", "gr"),
        P("tp"),
    )
    return jax.shard_map(
        shards,
        mesh=mesh,
        in_specs=placed,
        out_specs=(P("gr", "tp", None), P("gr", "tp")),
        check_vma=False,
    )
```

```python
import functools

import jax
import jax.numpy as jnp
import numpy as np
from jax import lax
from jax.experimental import pallas as pl
from jax.experimental.pallas import tpu as pltpu
from jax.sharding import PartitionSpec as P

HEAD_DIM = 64
PAIR = 2
MESH = pl.DeviceIdType.MESH
F32 = jnp.float32
HIGH = lax.Precision.HIGHEST


def kernel(
    sizes,
    tok, kw, vw, ld, cos_tab, sin_tab, nq_in, nk_in, nv_in, sd_in, gain_in,
    out, read,
    nq, nk, nv, sd, gain, staged, read_at, toks, w, lds, tots, wts, own_state, part, got, full, cos_ref, sin_ref, ends, qx, outer, decay, raw_ref, acc,
    l_sem, w_sem, yw_s, yw_r, tok_s, tok_r, core_s, core_r, z_s, z_r, x_s, x_r,
    ld_s, ld_r, tot_s, tot_r, z_h, rs_s, rs_r, ag_s, ag_r, yg_s, yg_r, ac_s, out_sem,
):
    n_sp, seqs, span, heads = sizes
    n_a = n_sp // 2
    g, sp, tp = lax.axis_index("gr"), lax.axis_index("sp"), lax.axis_index("tp")
    a, b = sp // 2, sp % 2
    ob = 1 - b
    core = tp % 2
    mate = tp + 1 - 2 * core
    rows, width = tok.shape
    depth = kw.shape[0]
    cols = kw.shape[1] // 2
    n_c = cols // 128
    last = n_c - 1
    pair_rows = PAIR * span
    pair_state = PAIR * HEAD_DIM
    hs = heads * seqs
    peer = a * 2 + ob
    y_peer = (g, peer, tp)
    x_peer = (1 - g, sp, tp)
    core_peer = (g, sp, mate)
    edge = jnp.logical_or(a == 0, a == n_a - 1)
    ahead = jnp.where(a < n_a // 2, 1, -1)

    barrier = pltpu.get_barrier_semaphore()

    @pl.loop(1, n_sp)
    def _(k):
        pl.semaphore_signal(barrier, inc=1, device_id=(g, lax.rem(sp + k, n_sp), tp), device_id_type=MESH)

    pl.semaphore_signal(barrier, inc=1, device_id=x_peer, device_id_type=MESH)
    pl.semaphore_signal(barrier, inc=1, device_id=core_peer, device_id_type=MESH)
    def lanes(m):
        return pl.ds(m * 128 if isinstance(m, int) else pl.multiple_of(m * 128, 128), 128)

    def columns(side, j):
        return pl.ds(pl.multiple_of(side * cols + j * 128, 128), 128)

    def shard_rows(s):
        return pl.ds(pl.multiple_of(s * depth, depth), depth)

    def own_weight(m, j):
        return pltpu.make_async_copy(
            (kw, vw)[m].at[:, columns(b, j)], w.at[j, shard_rows(sp), lanes(m)], w_sem.at[j]
        )

    local = [
        pltpu.make_async_copy(ld, lds.at[b], l_sem.at[0]),
        pltpu.make_async_copy(tok, toks.at[b], l_sem.at[1]),
        pltpu.make_async_copy(cos_tab.at[pl.ds(pl.multiple_of(a * 2 * span, 8), 2 * span)], cos_ref, l_sem.at[2]),
        pltpu.make_async_copy(sin_tab.at[pl.ds(pl.multiple_of(a * 2 * span, 8), 2 * span)], sin_ref, l_sem.at[3]),
        pltpu.make_async_copy(cos_tab.at[pl.ds(n_sp * span, 8)], ends.at[0], l_sem.at[4]),
        pltpu.make_async_copy(sin_tab.at[pl.ds(n_sp * span, 8)], ends.at[1], l_sem.at[5]),
        pltpu.make_async_copy(nq_in, nq, l_sem.at[6]),
        pltpu.make_async_copy(nk_in, nk, l_sem.at[7]),
        pltpu.make_async_copy(nv_in, nv, l_sem.at[8]),
        pltpu.make_async_copy(sd_in, sd, l_sem.at[9]),
        pltpu.make_async_copy(gain_in, gain, l_sem.at[10]),
    ]
    for j in range(n_c):
        for m in range(2):
            own_weight(m, j).start()
    for c in local:
        c.start()

    pl.semaphore_wait(barrier, n_sp + 1)

    def remote(src, dst, s, r, dev):
        return pltpu.make_async_remote_copy(
            src_ref=src, dst_ref=dst, send_sem=s, recv_sem=r, device_id=dev, device_id_type=MESH
        )

    def drain(ref, sem):
        pltpu.make_async_copy(ref, ref, sem).wait()

    def yw(m, j):
        return remote(
            (kw, vw)[m].at[:, columns(ob, j)], w.at[j, shard_rows(sp), lanes(m)], yw_s, yw_r.at[m, j], y_peer
        )

    def half_prompt(s):
        half = span // 2
        return pl.ds(pl.multiple_of(s * span + core * half, half), half)

    def ytok(h):
        return remote(tok.at[half_prompt(h)], toks.at[b, half_prompt(h)], tok_s, tok_r.at[h], y_peer)

    def ytok_in(h):
        here = toks.at[ob, half_prompt(h)]
        return remote(here, here, tok_s, tok_r.at[h], y_peer)

    def ctok(h):
        here = toks.at[ob, half_prompt(h)]
        return remote(here, here, core_s, core_r.at[h], core_peer)

    yld = remote(ld, lds.at[b], ld_s, ld_r, y_peer)

    early = min(2, n_c)
    soon = min(3, n_c)
    for m in range(2):
        @pl.when(g == m)
        def _():
            for j in range(early):
                yw(m, j).start()
            yld.start()
            for j in range(early):
                yw(1 - m, j).start()
            for j in range(early, soon):
                yw(m, j).start()
            for h in range(seqs // 2):
                ytok(h).start()
            for j in range(soon, n_c):
                yw(m, j).start()
            for j in range(early, last):
                yw(1 - m, j).start()
            for h in range(seqs // 2, seqs):
                ytok(h).start()
            for j in range(max(early, last), n_c):
                yw(1 - m, j).start()

    def yw_wait(m_is_g, j):
        for m in range(2):
            @pl.when(g == (m if m_is_g else 1 - m))
            def _():
                yw(m, j).wait_recv()

    def pieces(j, bb):
        return 2 if (j, bb) in ((0, 0), (last, 1)) else 1

    def piece(j, s, bb, q):
        size = depth // pieces(j, bb)
        return w.at[j, pl.ds(pl.multiple_of(s * depth + q * size, size), size), lanes(g)]

    def zsend(j, s, bb, q, t):
        ref = piece(j, s, bb, q)
        arrived = z_r.at[j, s] if q == 0 else z_h.at[bb, s // 2]
        return remote(ref, ref, z_s.at[(t + 1) // 2], arrived, (g, sp + 2 * t, tp))

    def xsend(j, s, bb, q):
        ref = piece(j, s, bb, q)
        return remote(ref, ref, x_s, x_r.at[j if j < last else last + s // 2], x_peer)

    def exists(place):
        return jnp.logical_and(place >= 0, place < n_a)

    def launch(j, s, bb):
        for t in (-ahead, ahead):
            @pl.when(exists(a + t))
            def _():
                for q in range(pieces(j, bb)):
                    zsend(j, s, bb, q, t).start()

    def start_own(j):
        drain(w.at[j, shard_rows(sp)], w_sem.at[j])
        launch(j, sp, 0)

    def start_chunk(j):
        if j >= early:
            start_own(j)
        yw_wait(True, j)
        launch(j, peer, 1)

    def zstep(j, d, bb):
        side = b if bb == 0 else ob
        for t in (ahead, -ahead):
            @pl.when(exists(a + t * d))
            def _():
                s = (a + t * d) * 2 + side
                for q in range(pieces(j, bb)):
                    zsend(j, s, bb, q, -t).wait_recv()

                    @pl.when(exists(a - t))
                    def _():
                        zsend(j, s, bb, q, -t).start()

                    xsend(j, s, bb, q).start()

    def gather_x(j):
        yw_wait(False, j)
        drain(w.at[j, pl.ds(0, 2 * (n_a - 1) * depth), lanes(0)], x_r.at[j])

    for j in range(early):
        start_own(j)
    def tsend(k):
        return remote(tots.at[a], tots.at[a], tot_s, tot_r.at[k], (g, lax.rem(a + k, n_a) * 2 + b, tp))

    for c in local:
        c.wait()
    raw_ref[...] = jnp.zeros(raw_ref.shape, F32)
    acc[...] = jnp.zeros(acc.shape, F32)
    tots[a] = jnp.zeros(tots.shape[1:], F32)

    def shard_total(tb):
        return lax.dot_general(
            jnp.ones((8, span), F32), lds[tb], (((1,), (1,)), ((), ())), precision=HIGH, preferred_element_type=F32
        )

    def total():
        yld.wait_recv()
        tots[a, :, 0:hs] = shard_total(0) + shard_total(1)

        @pl.loop(1, n_a)
        def _(k):
            tsend(k).start()

    lanes_at = lax.broadcasted_iota(jnp.int32, (HEAD_DIM, 128), 1)
    subs_at = lax.broadcasted_iota(jnp.int32, (HEAD_DIM, 128), 0)
    diagonal = lanes_at % HEAD_DIM == subs_at
    same_head = jnp.where(
        lax.broadcasted_iota(jnp.int32, (128, 128), 0) // HEAD_DIM
        == lax.broadcasted_iota(jnp.int32, (128, 128), 1) // HEAD_DIM, 1.0, 0.0
    ).astype(F32)

    def exact(x, y):
        return jnp.dot(x, y, precision=HIGH, preferred_element_type=F32)

    def at_end(u):
        low = lax.broadcasted_iota(jnp.int32, u.shape, 1) % HEAD_DIM < HEAD_DIM // 2
        turned = jnp.where(low, pltpu.roll(u, 128 - 32, 1), pltpu.roll(u, 32, 1))
        return u * ends[0, 0:1, :] + turned * ends[1, 0:1, :]

    head_lane = lax.broadcasted_iota(jnp.int32, (heads, 2 * cols), 1) // HEAD_DIM
    head_row = lax.broadcasted_iota(jnp.int32, (heads, 2 * cols), 0)
    spread_heads = jnp.where(head_lane == head_row, 1.0, 0.0).astype(F32)
    decay[...] = jnp.exp(exact(sd[...], spread_heads))

    def new_token(c0):
        chunk = pl.ds(c0, 128)
        query = at_end(nq[:, chunk].astype(F32)) * HEAD_DIM ** 0.5
        key_new = at_end(nk[:, chunk].astype(F32))
        value_new = nv[:, chunk].astype(F32)
        for s in range(seqs):
            at = pl.ds(s * HEAD_DIM, HEAD_DIM)
            qx[at, chunk] = exact(jnp.where(diagonal, query[s:s + 1], 0.0), same_head)
            column = exact(jnp.where(diagonal, key_new[s:s + 1], 0.0), same_head)
            outer[at, chunk] = column * value_new[s:s + 1]

    def weigh():
        @pl.loop(1, n_a)
        def _(k):
            tsend(k).wait_recv()

        pos_t = lax.broadcasted_iota(jnp.int32, (span, span), 0)
        pos_u = lax.broadcasted_iota(jnp.int32, (span, span), 1)
        later_mask = jnp.where(pos_u > pos_t, 1.0, 0.0).astype(F32)
        row_hs = lax.broadcasted_iota(jnp.int32, (hs, cols), 0)
        lane_head = lax.broadcasted_iota(jnp.int32, (hs, cols), 1) // HEAD_DIM + b * (heads // 2)

        def add(k, total):
            return total + jnp.where(k > a, tots[k], 0.0)

        after = lax.fori_loop(0, n_a, add, jnp.zeros(tots.shape[1:], F32))
        for tb in range(2):
            inside = lax.dot_general(
                later_mask, lds[tb], (((1,), (1,)), ((), ())), precision=HIGH, preferred_element_type=F32
            )
            suffix = inside + after[0:1, :hs]
            if tb == 0:
                suffix = suffix + shard_total(1)[0:1]
            for s in range(seqs):
                select = jnp.where(row_hs == lane_head * seqs + s, 1.0, 0.0).astype(F32)
                wts[tb, s] = jnp.exp(jnp.dot(suffix, select, precision=HIGH, preferred_element_type=F32))

    lane = lax.broadcasted_iota(jnp.int32, (span, 128), 1)
    first = lane % HEAD_DIM < HEAD_DIM // 2
    lane_out = lax.broadcasted_iota(jnp.int32, (HEAD_DIM, 128), 1)

    def states(tb, s, n, j):
        at = pl.ds(pl.multiple_of(s * span, span), n * span)
        return contract(jnp.dot(toks[tb, at, :], w[j], preferred_element_type=F32), tb, s, n, j)

    def contract(prod, tb, s, n, j):
        keys = prod[:, :128].astype(jnp.bfloat16).astype(F32)
        values = prod[:, 128:].astype(jnp.bfloat16)
        spot = pl.ds(pl.multiple_of(tb * span, span), span)
        result = []
        for i in range(n):
            u = keys[i * span:(i + 1) * span]
            turned = jnp.where(first, pltpu.roll(u, 128 - 32, 1), pltpu.roll(u, 32, 1))
            rk = u * cos_ref[spot, :] + turned * sin_ref[spot, :]
            weighted = (rk * wts[tb, s + i, :, pl.ds(j * 128, 128)]).astype(jnp.bfloat16)
            term = lax.dot_general(
                weighted, values[i * span:(i + 1) * span], (((0,), (0,)), ((), ())), preferred_element_type=F32
            )
            result.append(jnp.where(lane_out < HEAD_DIM, term[:HEAD_DIM], term[HEAD_DIM:]))
        return result

    late_rows = rows - span
    early_blocks = [(0, r, pair_rows) for r in range(0, rows, pair_rows)]
    early_blocks += [(1, r, min(pair_rows, late_rows - r)) for r in range(0, late_rows, pair_rows)]
    late_blocks = [(1, late_rows, span)]
    all_blocks = [(k, r, pair_rows) for k in range(2) for r in range(0, rows, pair_rows)]

    def accumulate(place, blocks):
        rows_at = pl.ds(pl.multiple_of(place * 2 * depth, 2 * depth), 2 * depth)
        for k, r, n in blocks:
            acc[k, r:r + n] += jnp.dot(
                toks[ob if k else b, r:r + n, rows_at], w[last, rows_at, :], preferred_element_type=F32
            )

    behind = jnp.where(ahead > 0, a, n_a - 1 - a)

    def place(i):
        paired = i < 2 * behind
        step = jnp.where(paired, i // 2 + 1, i - behind + 1)
        return a + jnp.where(jnp.logical_and(paired, i % 2 == 1), -ahead, ahead) * step

    def take(i, blocks):
        drain(w.at[last, pl.ds(0, 2 * depth), lanes(0)], x_r.at[last + place(i)])
        accumulate(place(i), blocks)

    def own(j):
        @pl.loop(0, seqs // PAIR)
        def _(p):
            for i, state in enumerate(states(b, p * PAIR, PAIR, j)):
                own_state[p * PAIR + i, j] = state

    def reducer(s, j):
        return n_a // 2 - 1 + (s + j) % 2

    def rs(s, j):
        to = reducer(s, j)
        return remote(part.at[s, j], got.at[a, s // 2, j], rs_s.at[(s + j) % 2], rs_r.at[s // 2, j], (g, to * 2 + b, tp))

    def partner(s, n, chunks):
        ready = [states(ob, s, n, j) for j in chunks]
        for j, of_chunk in zip(chunks, ready):
            for i in range(n):
                part[s + i, j] = (own_state[s + i, j] + of_chunk[i]).astype(jnp.bfloat16)
        for j in chunks:
            for i in range(n):
                rs_start(s + i, j)

    def rs_start(s, j):
        @pl.when(a != reducer(s, j))
        def _():
            rs(s, j).start()

    def ag(s, j, to):
        here = full.at[b, s, j]
        return remote(here, here, ag_s, ag_r.at[s, j], (g, to * 2 + b, tp))

    def direct(j):
        return j == last

    def across(s, j, to):
        here = full.at[b, s, j]
        return remote(here, here, ac_s, yg_r.at[s, j], (g, to * 2 + ob, tp))

    def yg(s, j, side):
        here = full.at[side, s, j]
        return remote(here, here, yg_s, yg_r.at[s, j], y_peer)

    def reduce(s, j):
        @pl.when(a == reducer(s, j))
        def _():
            drain(got.at[pl.ds(0, n_a - 1), s // 2, j], rs_r.at[s // 2, j])

            def add(k, total):
                return total + got[lax.rem(a + k, n_a), s // 2, j].astype(F32)

            total = lax.fori_loop(1, n_a, add, part[s, j].astype(F32))
            full[b, s, j] = total.astype(jnp.bfloat16)

            @pl.loop(1, n_a)
            def _(k):
                to = lax.rem(a + k, n_a)
                if direct(j):
                    across(s, j, to).start()
                ag(s, j, to).start()

            if direct(j):
                across(s, j, a).start()
            else:
                yg(s, j, b).start()

    def collect(s, j):
        @pl.when(a != reducer(s, j))
        def _():
            ag(s, j, a).wait_recv()
            if not direct(j):
                yg(s, j, b).start()

    def finish(side, p, j):
        chunk = columns(side, j)
        raws, done = [], []
        for i in range(PAIR):
            s = p * PAIR + i
            at = pl.ds(s * HEAD_DIM, HEAD_DIM)
            state = decay[s:s + 1, chunk] * full[side, s, j].astype(F32) + outer[at, chunk]
            raws.append(jnp.sum(qx[at, chunk] * state, axis=0, keepdims=True))
            done.append(state)
        staged[chunk, p * pair_state:(p + 1) * pair_state] = jnp.concatenate(done, axis=0).T
        raw_ref[side * n_c + j, p * PAIR:(p + 1) * PAIR, :] = jnp.concatenate(raws, axis=0)

    def put(side, j):
        return pltpu.make_async_copy(staged.at[columns(side, j)], out.at[columns(side, j)], out_sem)

    def tokens_in(s):
        ytok_in(s).wait_recv()
        ctok(s).start()

    def normalize(chunks):
        if not chunks:
            return
        raw = jnp.concatenate([raw_ref[c] for c in chunks], axis=0)
        off = raw - exact(raw, same_head) * (1.0 / HEAD_DIM)
        spread = exact(off * off, same_head) * (1.0 / HEAD_DIM)
        normed = off * lax.rsqrt(spread + 1e-06)
        for i, c in enumerate(chunks):
            chunk = pl.ds(c * 128, 128)
            read_at[:, chunk] = (normed[i * 8:i * 8 + seqs] * gain[:, chunk]).astype(jnp.bfloat16)

    new_chunks = list(range(0, 2 * cols, 128))
    for j in range(n_c):
        if j > 0:
            @pl.when(jnp.logical_not(edge))
            def _():
                start_chunk(j)

        turns = [[(j, step // 2 + 1, step % 2)] for step in range(6)]
        if early > 1 and j == 0:
            turns = [
                [(0, 1, 0)], [(1, 1, 0), (0, 2, 0)], [(0, 1, 1), (1, 2, 0)],
                [(0, 3, 0)], [(0, 2, 1), (1, 3, 0)], [(0, 3, 1)],
            ]
        if early > 1 and j == 1:
            turns = [[], [(1, 1, 1)], [(1, 2, 1)], [(1, 3, 1)], [], []]
        for step in range(6):
            for turn in turns[step]:
                zstep(*turn)
            if j == 0 and step == 0:
                start_chunk(0)
            if step == 2 and j < last:
                @pl.when(edge)
                def _():
                    start_chunk(j + 1)
            if j == 0:
                for c0 in new_chunks[step::4] if step < 4 else ():
                    new_token(c0)
                if step == 3:
                    total()
            else:
                if j == 1 and step == 1:
                    weigh()
                if j == last and step == 1:
                    for s in range(0 if last < 2 else seqs // 2, seqs - 1):
                        tokens_in(s)
                if step == 2:
                    gather_x(j - 1)
                    own(j - 1)
                if j == last - 1 and step == 3:
                    for s in range(seqs // 2):
                        tokens_in(s)
                if j == last - 1 and step == 4:
                    for s in range(seqs // 2):
                        ctok(s).wait_recv()
                    partner(0, PAIR, range(last - 1))
                if j == last and step == 3:
                    for s in range(0 if last < 2 else seqs // 2, seqs - 1):
                        ctok(s).wait_recv()
                    partner(0, PAIR, [last - 1])
                    for s in range(seqs // 2, seqs - 1):
                        partner(s, 1, [0])
                if j == last and step == 4:
                    for s in range(seqs // 2, seqs - 1):
                        partner(s, 1, range(1, last))
                    for s in range(seqs // 2):
                        for k in range(last - 1):
                            reduce(s, k)
                    tokens_in(seqs - 1)

        @pl.loop(4, n_a)
        def _(d):
            for bb in range(2):
                zstep(j, d, bb)

    if last == 0:
        weigh()
        for s in range(seqs):
            tokens_in(s)
        for s in range(seqs):
            ctok(s).wait_recv()
    take(0, early_blocks)
    take(1, early_blocks)
    yw_wait(False, last)
    accumulate(a, early_blocks)
    if last > 0:
        ctok(seqs - 1).wait_recv()
    partner(seqs - 1, 1, range(last))
    for s in range(seqs - 1):
        for k in range(last - 1 if s < seqs // 2 else 0, last):
            reduce(s, k)
    for s in range(seqs // 2):
        for k in range(last - 1):
            collect(s, k)
    accumulate(a, late_blocks)
    accumulate(place(0), late_blocks)
    accumulate(place(1), late_blocks)

    @pl.loop(2, n_a - 1)
    def _(i):
        take(i, all_blocks)

    sums = [contract(acc[0], b, 0, seqs, last), contract(acc[1], ob, 0, seqs, last)]
    for s in range(seqs):
        part[s, last] = (sums[0][s] + sums[1][s]).astype(jnp.bfloat16)
    for s in range(seqs):
        rs_start(s, last)
    for k in range(last):
        reduce(seqs - 1, k)
    for s in range(seqs):
        reduce(s, last)
    for s in range(seqs // 2):
        for k in range(max(last - 1, 0), last):
            collect(s, k)
    for s in range(seqs // 2, seqs):
        for k in range(last):
            collect(s, k)
    for j in range(last):
        for s in range(PAIR):
            yg(s, j, ob).wait_recv()
        finish(b, 0, j)
        finish(ob, 0, j)
    for j in range(last):
        for p in range(1, seqs // PAIR):
            for s in range(p * PAIR, (p + 1) * PAIR):
                yg(s, j, ob).wait_recv()
            finish(b, p, j)
            finish(ob, p, j)
        put(b, j).start()
        put(ob, j).start()
    normalize([side * n_c + j for side in range(2) for j in range(last)])
    for s in range(seqs):
        collect(s, last)
        yg(s, last, ob).wait_recv()
    for side in (b, ob):
        for p in range(seqs // PAIR):
            finish(side, p, last)
        put(side, last).start()
    normalize([side * n_c + last for side in range(2)])
    read_out = pltpu.make_async_copy(read_at, read, l_sem.at[0])
    read_out.start()

    for parity in range(2):
        @pl.when(a != reducer(parity, 0))
        def _():
            drain(part.at[pl.ds(0, seqs // 2)], rs_s.at[parity])

        @pl.when(a == reducer(parity, 0))
        def _():
            drain(got.at[pl.ds(0, n_a - 1)], ag_s)
            drain(got.at[:, :, 0], ac_s)

    if last > 0:
        drain(full.at[0, :, pl.ds(0, last)], yg_s)
    drain(toks.at[0, pl.ds(0, rows // 2)], tok_s)
    drain(toks.at[0, pl.ds(0, rows // 2)], core_s)
    drain(tots.at[pl.ds(0, n_a - 1)], tot_s)
    yld.wait_send()
    drain(w.at[:, pl.ds(0, depth)], yw_s)
    drain(w.at[:, pl.ds(0, 2 * (n_a - 1) * depth), lanes(0)], x_s)
    for k in range(n_a):
        @pl.when(a == k)
        def _():
            if k < n_a - 1:
                drain(w.at[:, pl.ds(0, 2 * (k + 1) * depth), lanes(0)], z_s.at[1])
            if k > 0:
                drain(w.at[:, pl.ds(0, 2 * (n_a - k) * depth), lanes(0)], z_s.at[0])

    drain(staged, out_sem)
    read_out.wait()


def store(state, read, out, read_out, sem):
    copies = [pltpu.make_async_copy(state, out, sem.at[0]), pltpu.make_async_copy(read, read_out, sem.at[1])]
    for c in copies:
        c.start()
    for c in copies:
        c.wait()


def prompt_states(token_rows, key_weight, value_weight, decays, cos, sin, step, seqs, span, heads, n_sp):
    rows, width = token_rows.shape
    depth, whole = key_weight.shape
    cols = whole // 2
    n_c = cols // 128
    last = n_c - 1
    n_a = n_sp // 2
    hs = heads * seqs
    state_rows = seqs * HEAD_DIM
    dma = pltpu.SemaphoreType.DMA
    bf16 = jnp.bfloat16
    hbm = pl.BlockSpec(memory_space=pl.ANY)
    operands = (token_rows, key_weight, value_weight, decays, cos, sin, *step)
    state, read = pl.pallas_call(
        functools.partial(kernel, (n_sp, seqs, span, heads)),
        out_shape=(
            pltpu.VMEM((whole, state_rows), F32),
            pltpu.VMEM((seqs, whole), bf16),
        ),
        in_specs=[hbm] * 11,
        out_specs=(hbm, hbm),
        scratch_shapes=[
            *(pltpu.VMEM(v.shape, v.dtype) for v in step),
            pltpu.VMEM((whole, state_rows), F32),
            pltpu.VMEM((seqs, whole), bf16),
            pltpu.VMEM((2, rows, width), bf16),
            pltpu.VMEM((n_c, n_sp * depth, 256), bf16),
            pltpu.VMEM((2, hs, span), F32),
            pltpu.VMEM((n_a, 8, 128), F32),
            pltpu.VMEM((2, seqs, span, cols), F32),
            pltpu.VMEM((seqs, n_c, HEAD_DIM, 128), F32),
            pltpu.VMEM((seqs, n_c, HEAD_DIM, 128), bf16),
            pltpu.VMEM((n_a, seqs // 2, n_c, HEAD_DIM, 128), bf16),
            pltpu.VMEM((2, seqs, n_c, HEAD_DIM, 128), bf16),
            pltpu.VMEM((2 * span, 128), F32),
            pltpu.VMEM((2 * span, 128), F32),
            pltpu.VMEM((2, 8, 128), F32),
            pltpu.VMEM((state_rows, whole), F32),
            pltpu.VMEM((state_rows, whole), F32),
            pltpu.VMEM((seqs, whole), F32),
            pltpu.VMEM((2 * n_c, 8, 128), F32),
            pltpu.VMEM((2, rows, 256), F32),
            dma((11,)), dma((n_c,)), dma, dma((2, n_c)),
            dma, dma((seqs,)), dma, dma((seqs,)),
            dma((2,)), dma((n_c, n_sp)), dma, dma((last + n_a,)),
            dma, dma, dma, dma((n_a,)), dma((2, n_a)),
            dma((2,)), dma((seqs // 2, n_c)), dma, dma((seqs, n_c)),
            dma, dma((seqs, n_c)), dma, dma,
        ],
        compiler_params=pltpu.CompilerParams(
            collective_id=0, has_side_effects=True, vmem_limit_bytes=40 * 1024 * 1024
        ),
    )(*[pltpu.with_memory_space_constraint(v, pltpu.HBM) for v in operands])
    return pl.pallas_call(
        store,
        out_shape=(pltpu.HBM(state.shape, state.dtype), pltpu.HBM(read.shape, read.dtype)),
        in_specs=[pl.BlockSpec(memory_space=pltpu.VMEM)] * 2,
        out_specs=(hbm, hbm),
        scratch_shapes=[dma((2,))],
        compiler_params=pltpu.CompilerParams(vmem_limit_bytes=8 * 1024 * 1024),
    )(*[pltpu.with_memory_space_constraint(v, pltpu.VMEM) for v in (state, read)])


def position_tables(length):
    half = HEAD_DIM // 2
    inverse = np.float32(10000.0) ** (-np.arange(half, dtype=np.float32) * np.float32(2.0 / HEAD_DIM))
    angles = np.arange(length + 8, dtype=np.float32)[:, None] * inverse[None, :].astype(np.float32)
    cosine = np.cos(angles.astype(np.float64)) * HEAD_DIM ** -0.5
    sine = np.sin(angles.astype(np.float64)) * HEAD_DIM ** -0.5
    cos = np.concatenate([cosine] * 4, axis=-1).astype(np.float32)
    sin = np.concatenate([-sine, sine] * 2, axis=-1).astype(np.float32)
    return cos, sin


def shards(
    tokens, key_weight, value_weight, log_decay, new_query, new_key, new_value, step_decay, norm_gain
):
    seqs, span, width = tokens.shape
    heads = key_weight.shape[1] // HEAD_DIM
    n_sp = lax.axis_size("sp")
    token_rows = tokens.reshape(seqs * span, width)
    decays = log_decay.reshape(heads * seqs, span)
    cos, sin = position_tables(span * n_sp)
    step = (new_query, new_key, new_value, step_decay.T, norm_gain.reshape(1, -1))
    state, read = prompt_states(
        token_rows, key_weight, value_weight, decays, jnp.asarray(cos), jnp.asarray(sin), step,
        seqs, span, heads, n_sp,
    )
    return (state.T.reshape(seqs * HEAD_DIM, heads, HEAD_DIM), read)


def solution(mesh):
    placed = (
        P("gr", "sp", None),
        P("sp", "tp"),
        P("sp", "tp"),
        P("tp", "gr", "sp"),
        P("gr", "tp"),
        P("gr", "tp"),
        P("gr", "tp"),
        P("tp", "gr"),
        P("tp"),
    )
    return jax.shard_map(
        shards,
        mesh=mesh,
        in_specs=placed,
        out_specs=(P("gr", "tp", None), P("gr", "tp")),
        check_vma=False,
    )
```

```python
import functools

import jax
import jax.numpy as jnp
import numpy as np
from jax import lax
from jax.experimental import pallas as pl
from jax.experimental.pallas import tpu as pltpu
from jax.sharding import PartitionSpec as P

HEAD_DIM = 64
PAIR = 2
MESH = pl.DeviceIdType.MESH
F32 = jnp.float32
HIGH = lax.Precision.HIGHEST


def kernel(
    sizes,
    tok, kw, vw, ld, cos_tab, sin_tab, nq_in, nk_in, nv_in, sd_in, gain_in,
    out, read,
    nq, nk, nv, sd, gain, staged, read_at, toks, w, lds, tots, wts, own_state, part, got, full, cos_ref, sin_ref, ends, qx, outer, decay, raw_ref, acc,
    l_sem, w_sem, yw_s, yw_r, tok_s, tok_r, core_s, core_r, z_s, z_r, x_s, x_r,
    ld_s, ld_r, tot_s, tot_r, z_h, rs_s, rs_r, ag_s, ag_r, yg_s, yg_r, ac_s, out_sem,
):
    n_sp, seqs, span, heads = sizes
    n_a = n_sp // 2
    g, sp, tp = lax.axis_index("gr"), lax.axis_index("sp"), lax.axis_index("tp")
    a, b = sp // 2, sp % 2
    ob = 1 - b
    core = tp % 2
    mate = tp + 1 - 2 * core
    rows, width = tok.shape
    depth = kw.shape[0]
    cols = kw.shape[1] // 2
    n_c = cols // 128
    last = n_c - 1
    pair_rows = PAIR * span
    pair_state = PAIR * HEAD_DIM
    hs = heads * seqs
    peer = a * 2 + ob
    y_peer = (g, peer, tp)
    x_peer = (1 - g, sp, tp)
    core_peer = (g, sp, mate)
    edge = jnp.logical_or(a == 0, a == n_a - 1)
    ahead = jnp.where(a < n_a // 2, 1, -1)

    barrier = pltpu.get_barrier_semaphore()

    @pl.loop(1, n_sp)
    def _(k):
        pl.semaphore_signal(barrier, inc=1, device_id=(g, lax.rem(sp + k, n_sp), tp), device_id_type=MESH)

    pl.semaphore_signal(barrier, inc=1, device_id=x_peer, device_id_type=MESH)
    pl.semaphore_signal(barrier, inc=1, device_id=core_peer, device_id_type=MESH)
    def lanes(m):
        return pl.ds(m * 128 if isinstance(m, int) else pl.multiple_of(m * 128, 128), 128)

    def columns(side, j):
        return pl.ds(pl.multiple_of(side * cols + j * 128, 128), 128)

    def shard_rows(s):
        return pl.ds(pl.multiple_of(s * depth, depth), depth)

    def own_weight(m, j):
        return pltpu.make_async_copy(
            (kw, vw)[m].at[:, columns(b, j)], w.at[j, shard_rows(sp), lanes(m)], w_sem.at[j]
        )

    local = [
        pltpu.make_async_copy(ld, lds.at[b], l_sem.at[0]),
        pltpu.make_async_copy(tok, toks.at[b], l_sem.at[1]),
        pltpu.make_async_copy(cos_tab.at[pl.ds(pl.multiple_of(a * 2 * span, 8), 2 * span)], cos_ref, l_sem.at[2]),
        pltpu.make_async_copy(sin_tab.at[pl.ds(pl.multiple_of(a * 2 * span, 8), 2 * span)], sin_ref, l_sem.at[3]),
        pltpu.make_async_copy(cos_tab.at[pl.ds(n_sp * span, 8)], ends.at[0], l_sem.at[4]),
        pltpu.make_async_copy(sin_tab.at[pl.ds(n_sp * span, 8)], ends.at[1], l_sem.at[5]),
        pltpu.make_async_copy(nq_in, nq, l_sem.at[6]),
        pltpu.make_async_copy(nk_in, nk, l_sem.at[7]),
        pltpu.make_async_copy(nv_in, nv, l_sem.at[8]),
        pltpu.make_async_copy(sd_in, sd, l_sem.at[9]),
        pltpu.make_async_copy(gain_in, gain, l_sem.at[10]),
    ]
    for j in range(n_c):
        for m in range(2):
            own_weight(m, j).start()
    for c in local:
        c.start()

    pl.semaphore_wait(barrier, n_sp + 1)

    def remote(src, dst, s, r, dev):
        return pltpu.make_async_remote_copy(
            src_ref=src, dst_ref=dst, send_sem=s, recv_sem=r, device_id=dev, device_id_type=MESH
        )

    def drain(ref, sem):
        pltpu.make_async_copy(ref, ref, sem).wait()

    def yw(m, j):
        return remote(
            (kw, vw)[m].at[:, columns(ob, j)], w.at[j, shard_rows(sp), lanes(m)], yw_s, yw_r.at[m, j], y_peer
        )

    def half_prompt(s):
        half = span // 2
        return pl.ds(pl.multiple_of(s * span + core * half, half), half)

    def ytok(h):
        return remote(tok.at[half_prompt(h)], toks.at[b, half_prompt(h)], tok_s, tok_r.at[h], y_peer)

    def ytok_in(h):
        here = toks.at[ob, half_prompt(h)]
        return remote(here, here, tok_s, tok_r.at[h], y_peer)

    def ctok(h):
        here = toks.at[ob, half_prompt(h)]
        return remote(here, here, core_s, core_r.at[h], core_peer)

    yld = remote(ld, lds.at[b], ld_s, ld_r, y_peer)

    early = min(2, n_c)
    soon = min(3, n_c)
    for m in range(2):
        @pl.when(g == m)
        def _():
            for j in range(early):
                yw(m, j).start()
            yld.start()
            for j in range(early):
                yw(1 - m, j).start()
            for j in range(early, soon):
                yw(m, j).start()
            for h in range(seqs // 2):
                ytok(h).start()
            for j in range(soon, n_c):
                yw(m, j).start()
            for j in range(early, last):
                yw(1 - m, j).start()
            for h in range(seqs // 2, seqs):
                ytok(h).start()
            for j in range(max(early, last), n_c):
                yw(1 - m, j).start()

    def yw_wait(m_is_g, j):
        for m in range(2):
            @pl.when(g == (m if m_is_g else 1 - m))
            def _():
                yw(m, j).wait_recv()

    def pieces(j, bb):
        return 2 if (j, bb) in ((0, 0), (last, 1)) else 1

    def piece(j, s, bb, q):
        size = depth // pieces(j, bb)
        return w.at[j, pl.ds(pl.multiple_of(s * depth + q * size, size), size), lanes(g)]

    def zsend(j, s, bb, q, t):
        ref = piece(j, s, bb, q)
        arrived = z_r.at[j, s] if q == 0 else z_h.at[bb, s // 2]
        return remote(ref, ref, z_s.at[(t + 1) // 2], arrived, (g, sp + 2 * t, tp))

    def xsend(j, s, bb, q):
        ref = piece(j, s, bb, q)
        return remote(ref, ref, x_s, x_r.at[j if j < last else last + s // 2], x_peer)

    def exists(place):
        return jnp.logical_and(place >= 0, place < n_a)

    def launch(j, s, bb):
        for t in (-ahead, ahead):
            @pl.when(exists(a + t))
            def _():
                for q in range(pieces(j, bb)):
                    zsend(j, s, bb, q, t).start()

    def start_own(j):
        drain(w.at[j, shard_rows(sp)], w_sem.at[j])
        launch(j, sp, 0)

    def start_chunk(j):
        if j >= early:
            start_own(j)
        yw_wait(True, j)
        launch(j, peer, 1)

    def zstep(j, d, bb):
        side = b if bb == 0 else ob
        for t in (ahead, -ahead):
            @pl.when(exists(a + t * d))
            def _():
                s = (a + t * d) * 2 + side
                for q in range(pieces(j, bb)):
                    zsend(j, s, bb, q, -t).wait_recv()

                    @pl.when(exists(a - t))
                    def _():
                        zsend(j, s, bb, q, -t).start()

                    xsend(j, s, bb, q).start()

    def gather_x(j):
        yw_wait(False, j)
        drain(w.at[j, pl.ds(0, 2 * (n_a - 1) * depth), lanes(0)], x_r.at[j])

    for j in range(early):
        start_own(j)
    def tsend(k):
        return remote(tots.at[a], tots.at[a], tot_s, tot_r.at[k], (g, lax.rem(a + k, n_a) * 2 + b, tp))

    for c in local:
        c.wait()
    raw_ref[...] = jnp.zeros(raw_ref.shape, F32)
    acc[...] = jnp.zeros(acc.shape, F32)
    tots[a] = jnp.zeros(tots.shape[1:], F32)

    def shard_total(tb):
        return lax.dot_general(
            jnp.ones((8, span), F32), lds[tb], (((1,), (1,)), ((), ())), precision=HIGH, preferred_element_type=F32
        )

    def total():
        yld.wait_recv()
        tots[a, :, 0:hs] = shard_total(0) + shard_total(1)

        @pl.loop(1, n_a)
        def _(k):
            tsend(k).start()

    lanes_at = lax.broadcasted_iota(jnp.int32, (HEAD_DIM, 128), 1)
    subs_at = lax.broadcasted_iota(jnp.int32, (HEAD_DIM, 128), 0)
    diagonal = lanes_at % HEAD_DIM == subs_at
    same_head = jnp.where(
        lax.broadcasted_iota(jnp.int32, (128, 128), 0) // HEAD_DIM
        == lax.broadcasted_iota(jnp.int32, (128, 128), 1) // HEAD_DIM, 1.0, 0.0
    ).astype(F32)

    def exact(x, y):
        return jnp.dot(x, y, precision=HIGH, preferred_element_type=F32)

    def at_end(u):
        low = lax.broadcasted_iota(jnp.int32, u.shape, 1) % HEAD_DIM < HEAD_DIM // 2
        turned = jnp.where(low, pltpu.roll(u, 128 - 32, 1), pltpu.roll(u, 32, 1))
        return u * ends[0, 0:1, :] + turned * ends[1, 0:1, :]

    head_lane = lax.broadcasted_iota(jnp.int32, (heads, 2 * cols), 1) // HEAD_DIM
    head_row = lax.broadcasted_iota(jnp.int32, (heads, 2 * cols), 0)
    spread_heads = jnp.where(head_lane == head_row, 1.0, 0.0).astype(F32)
    decay[...] = jnp.exp(exact(sd[...], spread_heads))

    def new_token(c0):
        chunk = pl.ds(c0, 128)
        query = at_end(nq[:, chunk].astype(F32)) * HEAD_DIM ** 0.5
        key_new = at_end(nk[:, chunk].astype(F32))
        value_new = nv[:, chunk].astype(F32)
        for s in range(seqs):
            at = pl.ds(s * HEAD_DIM, HEAD_DIM)
            qx[at, chunk] = exact(jnp.where(diagonal, query[s:s + 1], 0.0), same_head)
            column = exact(jnp.where(diagonal, key_new[s:s + 1], 0.0), same_head)
            outer[at, chunk] = column * value_new[s:s + 1]

    def weigh():
        @pl.loop(1, n_a)
        def _(k):
            tsend(k).wait_recv()

        pos_t = lax.broadcasted_iota(jnp.int32, (span, span), 0)
        pos_u = lax.broadcasted_iota(jnp.int32, (span, span), 1)
        later_mask = jnp.where(pos_u > pos_t, 1.0, 0.0).astype(F32)
        row_hs = lax.broadcasted_iota(jnp.int32, (hs, cols), 0)
        lane_head = lax.broadcasted_iota(jnp.int32, (hs, cols), 1) // HEAD_DIM + b * (heads // 2)

        def add(k, total):
            return total + jnp.where(k > a, tots[k], 0.0)

        after = lax.fori_loop(0, n_a, add, jnp.zeros(tots.shape[1:], F32))
        for tb in range(2):
            inside = lax.dot_general(
                later_mask, lds[tb], (((1,), (1,)), ((), ())), precision=HIGH, preferred_element_type=F32
            )
            suffix = inside + after[0:1, :hs]
            if tb == 0:
                suffix = suffix + shard_total(1)[0:1]
            for s in range(seqs):
                select = jnp.where(row_hs == lane_head * seqs + s, 1.0, 0.0).astype(F32)
                wts[tb, s] = jnp.exp(jnp.dot(suffix, select, precision=HIGH, preferred_element_type=F32))

    lane = lax.broadcasted_iota(jnp.int32, (span, 128), 1)
    first = lane % HEAD_DIM < HEAD_DIM // 2
    lane_out = lax.broadcasted_iota(jnp.int32, (HEAD_DIM, 128), 1)

    def states(tb, s, n, j):
        at = pl.ds(pl.multiple_of(s * span, span), n * span)
        return contract(jnp.dot(toks[tb, at, :], w[j], preferred_element_type=F32), tb, s, n, j)

    def contract(prod, tb, s, n, j):
        keys = prod[:, :128].astype(jnp.bfloat16).astype(F32)
        values = prod[:, 128:].astype(jnp.bfloat16)
        spot = pl.ds(pl.multiple_of(tb * span, span), span)
        result = []
        for i in range(n):
            u = keys[i * span:(i + 1) * span]
            turned = jnp.where(first, pltpu.roll(u, 128 - 32, 1), pltpu.roll(u, 32, 1))
            rk = u * cos_ref[spot, :] + turned * sin_ref[spot, :]
            weighted = (rk * wts[tb, s + i, :, pl.ds(j * 128, 128)]).astype(jnp.bfloat16)
            term = lax.dot_general(
                weighted, values[i * span:(i + 1) * span], (((0,), (0,)), ((), ())), preferred_element_type=F32
            )
            result.append(jnp.where(lane_out < HEAD_DIM, term[:HEAD_DIM], term[HEAD_DIM:]))
        return result

    late_rows = rows - span
    early_blocks = [(0, r, pair_rows) for r in range(0, rows, pair_rows)]
    early_blocks += [(1, r, min(pair_rows, late_rows - r)) for r in range(0, late_rows, pair_rows)]
    late_blocks = [(1, late_rows, span)]
    all_blocks = [(k, r, pair_rows) for k in range(2) for r in range(0, rows, pair_rows)]

    def accumulate(place, blocks):
        rows_at = pl.ds(pl.multiple_of(place * 2 * depth, 2 * depth), 2 * depth)
        for k, r, n in blocks:
            acc[k, r:r + n] += jnp.dot(
                toks[ob if k else b, r:r + n, rows_at], w[last, rows_at, :], preferred_element_type=F32
            )

    behind = jnp.where(ahead > 0, a, n_a - 1 - a)

    def place(i):
        paired = i < 2 * behind
        step = jnp.where(paired, i // 2 + 1, i - behind + 1)
        return a + jnp.where(jnp.logical_and(paired, i % 2 == 1), -ahead, ahead) * step

    def take(i, blocks):
        drain(w.at[last, pl.ds(0, 2 * depth), lanes(0)], x_r.at[last + place(i)])
        accumulate(place(i), blocks)

    def own(j):
        @pl.loop(0, seqs // PAIR)
        def _(p):
            for i, state in enumerate(states(b, p * PAIR, PAIR, j)):
                own_state[p * PAIR + i, j] = state

    def reducer(s, j):
        return n_a // 2 - 1 + (s + j) % 2

    def rs(s, j):
        to = reducer(s, j)
        return remote(part.at[s, j], got.at[a, s // 2, j], rs_s.at[(s + j) % 2], rs_r.at[s // 2, j], (g, to * 2 + b, tp))

    def partner(s, n, chunks):
        ready = [states(ob, s, n, j) for j in chunks]
        for j, of_chunk in zip(chunks, ready):
            for i in range(n):
                part[s + i, j] = (own_state[s + i, j] + of_chunk[i]).astype(jnp.bfloat16)
        for j in chunks:
            for i in range(n):
                rs_start(s + i, j)

    def rs_start(s, j):
        @pl.when(a != reducer(s, j))
        def _():
            rs(s, j).start()

    def ag(s, j, to):
        here = full.at[b, s, j]
        return remote(here, here, ag_s, ag_r.at[s, j], (g, to * 2 + b, tp))

    def direct(s, j):
        return j == last or s == seqs - 1

    def across(s, j, to):
        here = full.at[b, s, j]
        return remote(here, here, ac_s.at[0 if j == last else 1], yg_r.at[s, j], (g, to * 2 + ob, tp))

    def yg(s, j, side):
        here = full.at[side, s, j]
        return remote(here, here, yg_s, yg_r.at[s, j], y_peer)

    def reduce(s, j):
        @pl.when(a == reducer(s, j))
        def _():
            drain(got.at[pl.ds(0, n_a - 1), s // 2, j], rs_r.at[s // 2, j])

            def add(k, total):
                return total + got[lax.rem(a + k, n_a), s // 2, j].astype(F32)

            total = lax.fori_loop(1, n_a, add, part[s, j].astype(F32))
            full[b, s, j] = total.astype(jnp.bfloat16)

            @pl.loop(1, n_a)
            def _(k):
                to = lax.rem(a + k, n_a)
                if direct(s, j):
                    across(s, j, to).start()
                ag(s, j, to).start()

            if direct(s, j):
                across(s, j, a).start()
            else:
                yg(s, j, b).start()

    def collect(s, j):
        @pl.when(a != reducer(s, j))
        def _():
            ag(s, j, a).wait_recv()
            if not direct(s, j):
                yg(s, j, b).start()

    def finish(side, p, j):
        chunk = columns(side, j)
        raws, done = [], []
        for i in range(PAIR):
            s = p * PAIR + i
            at = pl.ds(s * HEAD_DIM, HEAD_DIM)
            state = decay[s:s + 1, chunk] * full[side, s, j].astype(F32) + outer[at, chunk]
            raws.append(jnp.sum(qx[at, chunk] * state, axis=0, keepdims=True))
            done.append(state)
        staged[chunk, p * pair_state:(p + 1) * pair_state] = jnp.concatenate(done, axis=0).T
        raw_ref[side * n_c + j, p * PAIR:(p + 1) * PAIR, :] = jnp.concatenate(raws, axis=0)

    def put(side, j):
        return pltpu.make_async_copy(staged.at[columns(side, j)], out.at[columns(side, j)], out_sem)

    def tokens_in(s):
        ytok_in(s).wait_recv()
        ctok(s).start()

    def normalize(chunks):
        if not chunks:
            return
        raw = jnp.concatenate([raw_ref[c] for c in chunks], axis=0)
        off = raw - exact(raw, same_head) * (1.0 / HEAD_DIM)
        spread = exact(off * off, same_head) * (1.0 / HEAD_DIM)
        normed = off * lax.rsqrt(spread + 1e-06)
        for i, c in enumerate(chunks):
            chunk = pl.ds(c * 128, 128)
            read_at[:, chunk] = (normed[i * 8:i * 8 + seqs] * gain[:, chunk]).astype(jnp.bfloat16)

    new_chunks = list(range(0, 2 * cols, 128))
    for j in range(n_c):
        if j > 0:
            @pl.when(jnp.logical_not(edge))
            def _():
                start_chunk(j)

        turns = [[(j, step // 2 + 1, step % 2)] for step in range(6)]
        if early > 1 and j == 0:
            turns = [
                [(0, 1, 0)], [(1, 1, 0), (0, 2, 0)], [(0, 1, 1), (1, 2, 0)],
                [(0, 3, 0)], [(0, 2, 1), (1, 3, 0)], [(0, 3, 1)],
            ]
        if early > 1 and j == 1:
            turns = [[], [(1, 1, 1)], [(1, 2, 1)], [(1, 3, 1)], [], []]
        for step in range(6):
            for turn in turns[step]:
                zstep(*turn)
            if j == 0 and step == 0:
                start_chunk(0)
            if step == 2 and j < last:
                @pl.when(edge)
                def _():
                    start_chunk(j + 1)
            if j == 0:
                for c0 in new_chunks[step::4] if step < 4 else ():
                    new_token(c0)
                if step == 3:
                    total()
            else:
                if j == 1 and step == 1:
                    weigh()
                if j == last and step == 1:
                    for s in range(0 if last < 2 else seqs // 2, seqs - 1):
                        tokens_in(s)
                if step == 2:
                    gather_x(j - 1)
                    own(j - 1)
                if j == last - 1 and step == 3:
                    for s in range(seqs // 2):
                        tokens_in(s)
                if j == last - 1 and step == 4:
                    for s in range(seqs // 2):
                        ctok(s).wait_recv()
                    partner(0, PAIR, range(last - 1))
                if j == last and step == 3:
                    for s in range(0 if last < 2 else seqs // 2, seqs - 1):
                        ctok(s).wait_recv()
                    partner(0, PAIR, [last - 1])
                    for s in range(seqs // 2, seqs - 1):
                        partner(s, 1, [0])
                if j == last and step == 4:
                    for s in range(seqs // 2, seqs - 1):
                        partner(s, 1, range(1, last))
                    for s in range(seqs // 2):
                        for k in range(last - 1):
                            reduce(s, k)
                    tokens_in(seqs - 1)

        @pl.loop(4, n_a)
        def _(d):
            for bb in range(2):
                zstep(j, d, bb)

    if last == 0:
        weigh()
        for s in range(seqs):
            tokens_in(s)
        for s in range(seqs):
            ctok(s).wait_recv()
    take(0, early_blocks)
    take(1, early_blocks)
    yw_wait(False, last)
    accumulate(a, early_blocks)
    for s in range(seqs - 1):
        for k in range(last - 1 if s < seqs // 2 else 0, last):
            reduce(s, k)
    if last > 0:
        ctok(seqs - 1).wait_recv()
    partner(seqs - 1, 1, range(last))
    for s in range(seqs // 2):
        for k in range(last - 1):
            collect(s, k)
    accumulate(a, late_blocks)
    accumulate(place(0), late_blocks)
    accumulate(place(1), late_blocks)

    @pl.loop(2, n_a - 1)
    def _(i):
        take(i, all_blocks)

    sums = [contract(acc[0], b, 0, seqs, last), contract(acc[1], ob, 0, seqs, last)]
    for s in range(seqs):
        part[s, last] = (sums[0][s] + sums[1][s]).astype(jnp.bfloat16)
    for s in range(seqs):
        rs_start(s, last)
    for s in range(seqs - 1):
        for k in range(last - 1 if s < seqs // 2 else 0, last):
            collect(s, k)
    for k in range(last):
        reduce(seqs - 1, k)
    for s in range(seqs):
        reduce(s, last)
    for k in range(last):
        collect(seqs - 1, k)
    for j in range(last):
        for s in range(PAIR):
            yg(s, j, ob).wait_recv()
        finish(b, 0, j)
        finish(ob, 0, j)
    for j in range(last):
        for p in range(1, seqs // PAIR):
            for s in range(p * PAIR, (p + 1) * PAIR):
                yg(s, j, ob).wait_recv()
            finish(b, p, j)
            finish(ob, p, j)
        put(b, j).start()
        put(ob, j).start()
    normalize([side * n_c + j for side in range(2) for j in range(last)])
    for s in range(seqs):
        collect(s, last)
        yg(s, last, ob).wait_recv()
    for side in (b, ob):
        for p in range(seqs // PAIR):
            finish(side, p, last)
        put(side, last).start()
    normalize([side * n_c + last for side in range(2)])
    read_out = pltpu.make_async_copy(read_at, read, l_sem.at[0])
    read_out.start()

    for parity in range(2):
        @pl.when(a != reducer(parity, 0))
        def _():
            drain(part.at[pl.ds(0, seqs // 2)], rs_s.at[parity])

        @pl.when(a == reducer(parity, 0))
        def _():
            drain(got.at[pl.ds(0, n_a - 1)], ag_s)
            drain(got.at[:, :, 0], ac_s.at[0])
            late = len([k for k in range(last) if (seqs - 1 + k) % 2 == parity])
            if late:
                drain(got.at[:, 0, pl.ds(0, late)], ac_s.at[1])

    if last > 0:
        drain(full.at[0, pl.ds(0, seqs - 1), pl.ds(0, last)], yg_s)
    drain(toks.at[0, pl.ds(0, rows // 2)], tok_s)
    drain(toks.at[0, pl.ds(0, rows // 2)], core_s)
    drain(tots.at[pl.ds(0, n_a - 1)], tot_s)
    yld.wait_send()
    drain(w.at[:, pl.ds(0, depth)], yw_s)
    drain(w.at[:, pl.ds(0, 2 * (n_a - 1) * depth), lanes(0)], x_s)
    for k in range(n_a):
        @pl.when(a == k)
        def _():
            if k < n_a - 1:
                drain(w.at[:, pl.ds(0, 2 * (k + 1) * depth), lanes(0)], z_s.at[1])
            if k > 0:
                drain(w.at[:, pl.ds(0, 2 * (n_a - k) * depth), lanes(0)], z_s.at[0])

    drain(staged, out_sem)
    read_out.wait()


def store(state, read, out, read_out, sem):
    copies = [pltpu.make_async_copy(state, out, sem.at[0]), pltpu.make_async_copy(read, read_out, sem.at[1])]
    for c in copies:
        c.start()
    for c in copies:
        c.wait()


def prompt_states(token_rows, key_weight, value_weight, decays, cos, sin, step, seqs, span, heads, n_sp):
    rows, width = token_rows.shape
    depth, whole = key_weight.shape
    cols = whole // 2
    n_c = cols // 128
    last = n_c - 1
    n_a = n_sp // 2
    hs = heads * seqs
    state_rows = seqs * HEAD_DIM
    dma = pltpu.SemaphoreType.DMA
    bf16 = jnp.bfloat16
    hbm = pl.BlockSpec(memory_space=pl.ANY)
    operands = (token_rows, key_weight, value_weight, decays, cos, sin, *step)
    state, read = pl.pallas_call(
        functools.partial(kernel, (n_sp, seqs, span, heads)),
        out_shape=(
            pltpu.VMEM((whole, state_rows), F32),
            pltpu.VMEM((seqs, whole), bf16),
        ),
        in_specs=[hbm] * 11,
        out_specs=(hbm, hbm),
        scratch_shapes=[
            *(pltpu.VMEM(v.shape, v.dtype) for v in step),
            pltpu.VMEM((whole, state_rows), F32),
            pltpu.VMEM((seqs, whole), bf16),
            pltpu.VMEM((2, rows, width), bf16),
            pltpu.VMEM((n_c, n_sp * depth, 256), bf16),
            pltpu.VMEM((2, hs, span), F32),
            pltpu.VMEM((n_a, 8, 128), F32),
            pltpu.VMEM((2, seqs, span, cols), F32),
            pltpu.VMEM((seqs, n_c, HEAD_DIM, 128), F32),
            pltpu.VMEM((seqs, n_c, HEAD_DIM, 128), bf16),
            pltpu.VMEM((n_a, seqs // 2, n_c, HEAD_DIM, 128), bf16),
            pltpu.VMEM((2, seqs, n_c, HEAD_DIM, 128), bf16),
            pltpu.VMEM((2 * span, 128), F32),
            pltpu.VMEM((2 * span, 128), F32),
            pltpu.VMEM((2, 8, 128), F32),
            pltpu.VMEM((state_rows, whole), F32),
            pltpu.VMEM((state_rows, whole), F32),
            pltpu.VMEM((seqs, whole), F32),
            pltpu.VMEM((2 * n_c, 8, 128), F32),
            pltpu.VMEM((2, rows, 256), F32),
            dma((11,)), dma((n_c,)), dma, dma((2, n_c)),
            dma, dma((seqs,)), dma, dma((seqs,)),
            dma((2,)), dma((n_c, n_sp)), dma, dma((last + n_a,)),
            dma, dma, dma, dma((n_a,)), dma((2, n_a)),
            dma((2,)), dma((seqs // 2, n_c)), dma, dma((seqs, n_c)),
            dma, dma((seqs, n_c)), dma((2,)), dma,
        ],
        compiler_params=pltpu.CompilerParams(
            collective_id=0, has_side_effects=True, vmem_limit_bytes=40 * 1024 * 1024
        ),
    )(*[pltpu.with_memory_space_constraint(v, pltpu.HBM) for v in operands])
    return pl.pallas_call(
        store,
        out_shape=(pltpu.HBM(state.shape, state.dtype), pltpu.HBM(read.shape, read.dtype)),
        in_specs=[pl.BlockSpec(memory_space=pltpu.VMEM)] * 2,
        out_specs=(hbm, hbm),
        scratch_shapes=[dma((2,))],
        compiler_params=pltpu.CompilerParams(vmem_limit_bytes=8 * 1024 * 1024),
    )(*[pltpu.with_memory_space_constraint(v, pltpu.VMEM) for v in (state, read)])


def position_tables(length):
    half = HEAD_DIM // 2
    inverse = np.float32(10000.0) ** (-np.arange(half, dtype=np.float32) * np.float32(2.0 / HEAD_DIM))
    angles = np.arange(length + 8, dtype=np.float32)[:, None] * inverse[None, :].astype(np.float32)
    cosine = np.cos(angles.astype(np.float64)) * HEAD_DIM ** -0.5
    sine = np.sin(angles.astype(np.float64)) * HEAD_DIM ** -0.5
    cos = np.concatenate([cosine] * 4, axis=-1).astype(np.float32)
    sin = np.concatenate([-sine, sine] * 2, axis=-1).astype(np.float32)
    return cos, sin


def shards(
    tokens, key_weight, value_weight, log_decay, new_query, new_key, new_value, step_decay, norm_gain
):
    seqs, span, width = tokens.shape
    heads = key_weight.shape[1] // HEAD_DIM
    n_sp = lax.axis_size("sp")
    token_rows = tokens.reshape(seqs * span, width)
    decays = log_decay.reshape(heads * seqs, span)
    cos, sin = position_tables(span * n_sp)
    step = (new_query, new_key, new_value, step_decay.T, norm_gain.reshape(1, -1))
    state, read = prompt_states(
        token_rows, key_weight, value_weight, decays, jnp.asarray(cos), jnp.asarray(sin), step,
        seqs, span, heads, n_sp,
    )
    return (state.T.reshape(seqs * HEAD_DIM, heads, HEAD_DIM), read)


def solution(mesh):
    placed = (
        P("gr", "sp", None),
        P("sp", "tp"),
        P("sp", "tp"),
        P("tp", "gr", "sp"),
        P("gr", "tp"),
        P("gr", "tp"),
        P("gr", "tp"),
        P("tp", "gr"),
        P("tp"),
    )
    return jax.shard_map(
        shards,
        mesh=mesh,
        in_specs=placed,
        out_specs=(P("gr", "tp", None), P("gr", "tp")),
        check_vma=False,
    )
```

```python
import functools

import jax
import jax.numpy as jnp
import numpy as np
from jax import lax
from jax.experimental import pallas as pl
from jax.experimental.pallas import tpu as pltpu
from jax.sharding import PartitionSpec as P

HEAD_DIM = 64
PAIR = 2
MESH = pl.DeviceIdType.MESH
F32 = jnp.float32
HIGH = lax.Precision.HIGHEST


def kernel(
    sizes,
    tok, kw, vw, ld, cos_tab, sin_tab, nq_in, nk_in, nv_in, sd_in, gain_in,
    out, read,
    nq, nk, nv, sd, gain, staged, read_at, toks, w, lds, tots, wts, own_state, part, got, full, cos_ref, sin_ref, ends, qx, outer, decay, raw_ref, acc,
    l_sem, w_sem, yw_s, yw_r, tok_s, tok_r, core_s, core_r, z_s, z_r, x_s, x_r,
    ld_s, ld_r, tot_s, tot_r, z_h, rs_s, rs_r, ag_s, ag_r, yg_s, yg_r, ac_s, out_sem,
):
    n_sp, seqs, span, heads = sizes
    n_a = n_sp // 2
    g, sp, tp = lax.axis_index("gr"), lax.axis_index("sp"), lax.axis_index("tp")
    a, b = sp // 2, sp % 2
    ob = 1 - b
    core = tp % 2
    mate = tp + 1 - 2 * core
    rows, width = tok.shape
    depth = kw.shape[0]
    cols = kw.shape[1] // 2
    n_c = cols // 128
    last = n_c - 1
    pair_rows = PAIR * span
    pair_state = PAIR * HEAD_DIM
    hs = heads * seqs
    peer = a * 2 + ob
    y_peer = (g, peer, tp)
    x_peer = (1 - g, sp, tp)
    core_peer = (g, sp, mate)
    edge = jnp.logical_or(a == 0, a == n_a - 1)
    ahead = jnp.where(a < n_a // 2, 1, -1)

    barrier = pltpu.get_barrier_semaphore()

    @pl.loop(1, n_sp)
    def _(k):
        pl.semaphore_signal(barrier, inc=1, device_id=(g, lax.rem(sp + k, n_sp), tp), device_id_type=MESH)

    pl.semaphore_signal(barrier, inc=1, device_id=x_peer, device_id_type=MESH)
    pl.semaphore_signal(barrier, inc=1, device_id=core_peer, device_id_type=MESH)
    def lanes(m):
        return pl.ds(m * 128 if isinstance(m, int) else pl.multiple_of(m * 128, 128), 128)

    def columns(side, j):
        return pl.ds(pl.multiple_of(side * cols + j * 128, 128), 128)

    def shard_rows(s):
        return pl.ds(pl.multiple_of(s * depth, depth), depth)

    def own_weight(m, j):
        return pltpu.make_async_copy(
            (kw, vw)[m].at[:, columns(b, j)], w.at[j, shard_rows(sp), lanes(m)], w_sem.at[j]
        )

    local = [
        pltpu.make_async_copy(ld, lds.at[b], l_sem.at[0]),
        pltpu.make_async_copy(tok, toks.at[b], l_sem.at[1]),
        pltpu.make_async_copy(cos_tab.at[pl.ds(pl.multiple_of(a * 2 * span, 8), 2 * span)], cos_ref, l_sem.at[2]),
        pltpu.make_async_copy(sin_tab.at[pl.ds(pl.multiple_of(a * 2 * span, 8), 2 * span)], sin_ref, l_sem.at[3]),
        pltpu.make_async_copy(cos_tab.at[pl.ds(n_sp * span, 8)], ends.at[0], l_sem.at[4]),
        pltpu.make_async_copy(sin_tab.at[pl.ds(n_sp * span, 8)], ends.at[1], l_sem.at[5]),
        pltpu.make_async_copy(nq_in, nq, l_sem.at[6]),
        pltpu.make_async_copy(nk_in, nk, l_sem.at[7]),
        pltpu.make_async_copy(nv_in, nv, l_sem.at[8]),
        pltpu.make_async_copy(sd_in, sd, l_sem.at[9]),
        pltpu.make_async_copy(gain_in, gain, l_sem.at[10]),
    ]
    for j in range(n_c):
        for m in range(2):
            own_weight(m, j).start()
    for c in local:
        c.start()

    pl.semaphore_wait(barrier, n_sp + 1)

    def remote(src, dst, s, r, dev):
        return pltpu.make_async_remote_copy(
            src_ref=src, dst_ref=dst, send_sem=s, recv_sem=r, device_id=dev, device_id_type=MESH
        )

    def drain(ref, sem):
        pltpu.make_async_copy(ref, ref, sem).wait()

    def yw(m, j):
        return remote(
            (kw, vw)[m].at[:, columns(ob, j)], w.at[j, shard_rows(sp), lanes(m)], yw_s, yw_r.at[m, j], y_peer
        )

    def half_prompt(s):
        half = span // 2
        return pl.ds(pl.multiple_of(s * span + core * half, half), half)

    def ytok(h):
        return remote(tok.at[half_prompt(h)], toks.at[b, half_prompt(h)], tok_s, tok_r.at[h], y_peer)

    def ytok_in(h):
        here = toks.at[ob, half_prompt(h)]
        return remote(here, here, tok_s, tok_r.at[h], y_peer)

    def ctok(h):
        here = toks.at[ob, half_prompt(h)]
        return remote(here, here, core_s, core_r.at[h], core_peer)

    yld = remote(ld, lds.at[b], ld_s, ld_r, y_peer)

    early = min(2, n_c)
    soon = min(3, n_c)
    for m in range(2):
        @pl.when(g == m)
        def _():
            for j in range(early):
                yw(m, j).start()
            yld.start()
            for j in range(early):
                yw(1 - m, j).start()
            for j in range(early, soon):
                yw(m, j).start()
            for h in range(seqs // 2):
                ytok(h).start()
            for j in range(soon, n_c):
                yw(m, j).start()
            for j in range(early, last):
                yw(1 - m, j).start()
            for h in range(seqs // 2, seqs):
                ytok(h).start()
            for j in range(max(early, last), n_c):
                yw(1 - m, j).start()

    def yw_wait(m_is_g, j):
        for m in range(2):
            @pl.when(g == (m if m_is_g else 1 - m))
            def _():
                yw(m, j).wait_recv()

    def pieces(j, bb):
        return 2 if (j, bb) in ((0, 0), (last, 1)) else 1

    def piece(j, s, bb, q):
        size = depth // pieces(j, bb)
        return w.at[j, pl.ds(pl.multiple_of(s * depth + q * size, size), size), lanes(g)]

    def zsend(j, s, bb, q, t):
        ref = piece(j, s, bb, q)
        arrived = z_r.at[j, s] if q == 0 else z_h.at[bb, s // 2]
        return remote(ref, ref, z_s.at[(t + 1) // 2], arrived, (g, sp + 2 * t, tp))

    def xsend(j, s, bb, q):
        ref = piece(j, s, bb, q)
        return remote(ref, ref, x_s, x_r.at[j if j < last else last + s // 2], x_peer)

    def exists(place):
        return jnp.logical_and(place >= 0, place < n_a)

    def launch(j, s, bb):
        for t in (-ahead, ahead):
            @pl.when(exists(a + t))
            def _():
                for q in range(pieces(j, bb)):
                    zsend(j, s, bb, q, t).start()

    def start_own(j):
        drain(w.at[j, shard_rows(sp)], w_sem.at[j])
        launch(j, sp, 0)

    def start_chunk(j):
        if j >= early:
            start_own(j)
        yw_wait(True, j)
        launch(j, peer, 1)

    def zstep(j, d, bb):
        side = b if bb == 0 else ob
        for t in (ahead, -ahead):
            @pl.when(exists(a + t * d))
            def _():
                s = (a + t * d) * 2 + side
                for q in range(pieces(j, bb)):
                    zsend(j, s, bb, q, -t).wait_recv()

                    @pl.when(exists(a - t))
                    def _():
                        zsend(j, s, bb, q, -t).start()

                    xsend(j, s, bb, q).start()

    def gather_x(j):
        yw_wait(False, j)
        drain(w.at[j, pl.ds(0, 2 * (n_a - 1) * depth), lanes(0)], x_r.at[j])

    for j in range(early):
        start_own(j)
    def tsend(k):
        return remote(tots.at[a], tots.at[a], tot_s, tot_r.at[k], (g, lax.rem(a + k, n_a) * 2 + b, tp))

    for c in local:
        c.wait()
    raw_ref[...] = jnp.zeros(raw_ref.shape, F32)
    acc[...] = jnp.zeros(acc.shape, F32)
    tots[a] = jnp.zeros(tots.shape[1:], F32)

    def shard_total(tb):
        return lax.dot_general(
            jnp.ones((8, span), F32), lds[tb], (((1,), (1,)), ((), ())), precision=HIGH, preferred_element_type=F32
        )

    def total():
        yld.wait_recv()
        tots[a, :, 0:hs] = shard_total(0) + shard_total(1)

        @pl.loop(1, n_a)
        def _(k):
            tsend(k).start()

    lanes_at = lax.broadcasted_iota(jnp.int32, (HEAD_DIM, 128), 1)
    subs_at = lax.broadcasted_iota(jnp.int32, (HEAD_DIM, 128), 0)
    diagonal = lanes_at % HEAD_DIM == subs_at
    same_head = jnp.where(
        lax.broadcasted_iota(jnp.int32, (128, 128), 0) // HEAD_DIM
        == lax.broadcasted_iota(jnp.int32, (128, 128), 1) // HEAD_DIM, 1.0, 0.0
    ).astype(F32)

    def exact(x, y):
        return jnp.dot(x, y, precision=HIGH, preferred_element_type=F32)

    def at_end(u):
        low = lax.broadcasted_iota(jnp.int32, u.shape, 1) % HEAD_DIM < HEAD_DIM // 2
        turned = jnp.where(low, pltpu.roll(u, 128 - 32, 1), pltpu.roll(u, 32, 1))
        return u * ends[0, 0:1, :] + turned * ends[1, 0:1, :]

    head_lane = lax.broadcasted_iota(jnp.int32, (heads, 2 * cols), 1) // HEAD_DIM
    head_row = lax.broadcasted_iota(jnp.int32, (heads, 2 * cols), 0)
    spread_heads = jnp.where(head_lane == head_row, 1.0, 0.0).astype(F32)
    decay[...] = jnp.exp(exact(sd[...], spread_heads))

    def new_token(c0):
        chunk = pl.ds(c0, 128)
        query = at_end(nq[:, chunk].astype(F32)) * HEAD_DIM ** 0.5
        key_new = at_end(nk[:, chunk].astype(F32))
        value_new = nv[:, chunk].astype(F32)
        for s in range(seqs):
            at = pl.ds(s * HEAD_DIM, HEAD_DIM)
            qx[at, chunk] = exact(jnp.where(diagonal, query[s:s + 1], 0.0), same_head)
            column = exact(jnp.where(diagonal, key_new[s:s + 1], 0.0), same_head)
            outer[at, chunk] = column * value_new[s:s + 1]

    def weigh():
        @pl.loop(1, n_a)
        def _(k):
            tsend(k).wait_recv()

        pos_t = lax.broadcasted_iota(jnp.int32, (span, span), 0)
        pos_u = lax.broadcasted_iota(jnp.int32, (span, span), 1)
        later_mask = jnp.where(pos_u > pos_t, 1.0, 0.0).astype(F32)
        row_hs = lax.broadcasted_iota(jnp.int32, (hs, cols), 0)
        lane_head = lax.broadcasted_iota(jnp.int32, (hs, cols), 1) // HEAD_DIM + b * (heads // 2)

        def add(k, total):
            return total + jnp.where(k > a, tots[k], 0.0)

        after = lax.fori_loop(0, n_a, add, jnp.zeros(tots.shape[1:], F32))
        for tb in range(2):
            inside = lax.dot_general(
                later_mask, lds[tb], (((1,), (1,)), ((), ())), precision=HIGH, preferred_element_type=F32
            )
            suffix = inside + after[0:1, :hs]
            if tb == 0:
                suffix = suffix + shard_total(1)[0:1]
            for s in range(seqs):
                select = jnp.where(row_hs == lane_head * seqs + s, 1.0, 0.0).astype(F32)
                wts[tb, s] = jnp.exp(jnp.dot(suffix, select, precision=HIGH, preferred_element_type=F32))

    lane = lax.broadcasted_iota(jnp.int32, (span, 128), 1)
    first = lane % HEAD_DIM < HEAD_DIM // 2
    lane_out = lax.broadcasted_iota(jnp.int32, (HEAD_DIM, 128), 1)

    def states(tb, s, n, j):
        at = pl.ds(pl.multiple_of(s * span, span), n * span)
        return contract(jnp.dot(toks[tb, at, :], w[j], preferred_element_type=F32), tb, s, n, j)

    def contract(prod, tb, s, n, j):
        keys = prod[:, :128].astype(jnp.bfloat16).astype(F32)
        values = prod[:, 128:].astype(jnp.bfloat16)
        spot = pl.ds(pl.multiple_of(tb * span, span), span)
        result = []
        for i in range(n):
            u = keys[i * span:(i + 1) * span]
            turned = jnp.where(first, pltpu.roll(u, 128 - 32, 1), pltpu.roll(u, 32, 1))
            rk = u * cos_ref[spot, :] + turned * sin_ref[spot, :]
            weighted = (rk * wts[tb, s + i, :, pl.ds(j * 128, 128)]).astype(jnp.bfloat16)
            term = lax.dot_general(
                weighted, values[i * span:(i + 1) * span], (((0,), (0,)), ((), ())), preferred_element_type=F32
            )
            result.append(jnp.where(lane_out < HEAD_DIM, term[:HEAD_DIM], term[HEAD_DIM:]))
        return result

    late_rows = rows - span
    early_blocks = [(0, r, pair_rows) for r in range(0, rows, pair_rows)]
    early_blocks += [(1, r, min(pair_rows, late_rows - r)) for r in range(0, late_rows, pair_rows)]
    late_blocks = [(1, late_rows, span)]
    all_blocks = [(k, r, pair_rows) for k in range(2) for r in range(0, rows, pair_rows)]

    def accumulate(place, blocks):
        rows_at = pl.ds(pl.multiple_of(place * 2 * depth, 2 * depth), 2 * depth)
        for k, r, n in blocks:
            acc[k, r:r + n] += jnp.dot(
                toks[ob if k else b, r:r + n, rows_at], w[last, rows_at, :], preferred_element_type=F32
            )

    behind = jnp.where(ahead > 0, a, n_a - 1 - a)

    def place(i):
        paired = i < 2 * behind
        step = jnp.where(paired, i // 2 + 1, i - behind + 1)
        return a + jnp.where(jnp.logical_and(paired, i % 2 == 1), -ahead, ahead) * step

    def take(i, blocks):
        drain(w.at[last, pl.ds(0, 2 * depth), lanes(0)], x_r.at[last + place(i)])
        accumulate(place(i), blocks)

    def own(j):
        @pl.loop(0, seqs // PAIR)
        def _(p):
            for i, state in enumerate(states(b, p * PAIR, PAIR, j)):
                own_state[p * PAIR + i, j] = state

    def reducer(s, j):
        return n_a // 2 - 1 + (s + j) % 2

    def rs(s, j):
        to = reducer(s, j)
        return remote(part.at[s, j], got.at[a, s // 2, j], rs_s.at[(s + j) % 2], rs_r.at[s // 2, j], (g, to * 2 + b, tp))

    def partner(s, n, chunks):
        ready = [states(ob, s, n, j) for j in chunks]
        for j, of_chunk in zip(chunks, ready):
            for i in range(n):
                part[s + i, j] = (own_state[s + i, j] + of_chunk[i]).astype(jnp.bfloat16)
        for j in chunks:
            for i in range(n):
                rs_start(s + i, j)

    def rs_start(s, j):
        @pl.when(a != reducer(s, j))
        def _():
            rs(s, j).start()

    def ag(s, j, to):
        here = full.at[b, s, j]
        return remote(here, here, ag_s, ag_r.at[s, j], (g, to * 2 + b, tp))

    def direct(s, j):
        return j == last or s == seqs - 1

    def across(s, j, to):
        here = full.at[b, s, j]
        return remote(here, here, ac_s.at[0 if j == last else 1], yg_r.at[s, j], (g, to * 2 + ob, tp))

    def yg(s, j, side):
        here = full.at[side, s, j]
        return remote(here, here, yg_s, yg_r.at[s, j], y_peer)

    def reduce(s, j):
        @pl.when(a == reducer(s, j))
        def _():
            drain(got.at[pl.ds(0, n_a - 1), s // 2, j], rs_r.at[s // 2, j])

            def add(k, total):
                return total + got[lax.rem(a + k, n_a), s // 2, j].astype(F32)

            total = lax.fori_loop(1, n_a, add, part[s, j].astype(F32))
            full[b, s, j] = total.astype(jnp.bfloat16)

            @pl.loop(1, n_a)
            def _(k):
                to = lax.rem(a + k, n_a)
                ag(s, j, to).start()
                if direct(s, j):
                    across(s, j, to).start()

            if direct(s, j):
                across(s, j, a).start()
            else:
                yg(s, j, b).start()

    def collect(s, j):
        @pl.when(a != reducer(s, j))
        def _():
            ag(s, j, a).wait_recv()
            if not direct(s, j):
                yg(s, j, b).start()

    def finish(side, p, j):
        chunk = columns(side, j)
        raws, done = [], []
        for i in range(PAIR):
            s = p * PAIR + i
            at = pl.ds(s * HEAD_DIM, HEAD_DIM)
            state = decay[s:s + 1, chunk] * full[side, s, j].astype(F32) + outer[at, chunk]
            raws.append(jnp.sum(qx[at, chunk] * state, axis=0, keepdims=True))
            done.append(state)
        staged[chunk, p * pair_state:(p + 1) * pair_state] = jnp.concatenate(done, axis=0).T
        raw_ref[side * n_c + j, p * PAIR:(p + 1) * PAIR, :] = jnp.concatenate(raws, axis=0)

    def put(side, j):
        return pltpu.make_async_copy(staged.at[columns(side, j)], out.at[columns(side, j)], out_sem)

    def tokens_in(s):
        ytok_in(s).wait_recv()
        ctok(s).start()

    def normalize(chunks):
        if not chunks:
            return
        raw = jnp.concatenate([raw_ref[c] for c in chunks], axis=0)
        off = raw - exact(raw, same_head) * (1.0 / HEAD_DIM)
        spread = exact(off * off, same_head) * (1.0 / HEAD_DIM)
        normed = off * lax.rsqrt(spread + 1e-06)
        for i, c in enumerate(chunks):
            chunk = pl.ds(c * 128, 128)
            read_at[:, chunk] = (normed[i * 8:i * 8 + seqs] * gain[:, chunk]).astype(jnp.bfloat16)

    new_chunks = list(range(0, 2 * cols, 128))
    for j in range(n_c):
        if j > 0:
            @pl.when(jnp.logical_not(edge))
            def _():
                start_chunk(j)

        turns = [[(j, step // 2 + 1, step % 2)] for step in range(6)]
        if early > 1 and j == 0:
            turns = [
                [(0, 1, 0)], [(1, 1, 0), (0, 2, 0)], [(0, 1, 1), (1, 2, 0)],
                [(0, 3, 0)], [(0, 2, 1), (1, 3, 0)], [(0, 3, 1)],
            ]
        if early > 1 and j == 1:
            turns = [[], [(1, 1, 1)], [(1, 2, 1)], [(1, 3, 1)], [], []]
        for step in range(6):
            for turn in turns[step]:
                zstep(*turn)
            if j == 0 and step == 0:
                start_chunk(0)
            if step == 2 and j < last:
                @pl.when(edge)
                def _():
                    start_chunk(j + 1)
            if j == 0:
                for c0 in new_chunks[step::4] if step < 4 else ():
                    new_token(c0)
                if step == 3:
                    total()
            else:
                if j == 1 and step == 1:
                    weigh()
                if j == last and step == 1:
                    for s in range(0 if last < 2 else seqs // 2, seqs - 1):
                        tokens_in(s)
                if step == 2:
                    gather_x(j - 1)
                    own(j - 1)
                if j == last - 1 and step == 3:
                    for s in range(seqs // 2):
                        tokens_in(s)
                if j == last - 1 and step == 4:
                    for s in range(seqs // 2):
                        ctok(s).wait_recv()
                    partner(0, PAIR, range(last - 1))
                if j == last and step == 3:
                    for s in range(0 if last < 2 else seqs // 2, seqs - 1):
                        ctok(s).wait_recv()
                    partner(0, PAIR, [last - 1])
                    for s in range(seqs // 2, seqs - 1):
                        partner(s, 1, [0])
                if j == last and step == 4:
                    for s in range(seqs // 2, seqs - 1):
                        partner(s, 1, range(1, last))
                    for s in range(seqs // 2):
                        for k in range(last - 1):
                            reduce(s, k)
                    take(0, early_blocks)
                    tokens_in(seqs - 1)

        @pl.loop(4, n_a)
        def _(d):
            for bb in range(2):
                zstep(j, d, bb)

    if last == 0:
        weigh()
        for s in range(seqs):
            tokens_in(s)
        for s in range(seqs):
            ctok(s).wait_recv()
    if last == 0:
        take(0, early_blocks)
    take(1, early_blocks)
    yw_wait(False, last)
    accumulate(a, early_blocks)
    for s in range(seqs - 1):
        for k in range(last - 1 if s < seqs // 2 else 0, last):
            reduce(s, k)
    if last > 0:
        ctok(seqs - 1).wait_recv()
    partner(seqs - 1, 1, range(last))
    for s in range(seqs // 2):
        for k in range(last - 1):
            collect(s, k)
    accumulate(a, late_blocks)
    accumulate(place(0), late_blocks)
    accumulate(place(1), late_blocks)

    @pl.loop(2, n_a - 1)
    def _(i):
        take(i, all_blocks)

    sums = [contract(acc[0], b, 0, seqs, last), contract(acc[1], ob, 0, seqs, last)]
    for s in range(seqs):
        part[s, last] = (sums[0][s] + sums[1][s]).astype(jnp.bfloat16)
    for s in range(seqs):
        rs_start(s, last)
    for s in range(seqs - 1):
        for k in range(last - 1 if s < seqs // 2 else 0, last):
            collect(s, k)
    for k in range(last):
        reduce(seqs - 1, k)
    for s in range(seqs):
        reduce(s, last)
    for k in range(last):
        collect(seqs - 1, k)
    for j in range(last):
        for s in range(PAIR):
            yg(s, j, ob).wait_recv()
        finish(b, 0, j)
        finish(ob, 0, j)
    for j in range(last):
        for p in range(1, seqs // PAIR):
            for s in range(p * PAIR, (p + 1) * PAIR):
                yg(s, j, ob).wait_recv()
            finish(b, p, j)
            finish(ob, p, j)
        put(b, j).start()
        put(ob, j).start()
    normalize([side * n_c + j for side in range(2) for j in range(last)])
    for s in range(seqs):
        collect(s, last)
    for p in range(seqs // PAIR):
        finish(b, p, last)
    put(b, last).start()
    for s in range(seqs):
        yg(s, last, ob).wait_recv()
    for p in range(seqs // PAIR):
        finish(ob, p, last)
    put(ob, last).start()
    normalize([side * n_c + last for side in range(2)])
    read_out = pltpu.make_async_copy(read_at, read, l_sem.at[0])
    read_out.start()

    for parity in range(2):
        @pl.when(a != reducer(parity, 0))
        def _():
            drain(part.at[pl.ds(0, seqs // 2)], rs_s.at[parity])

        @pl.when(a == reducer(parity, 0))
        def _():
            drain(got.at[pl.ds(0, n_a - 1)], ag_s)
            drain(got.at[:, :, 0], ac_s.at[0])
            late = len([k for k in range(last) if (seqs - 1 + k) % 2 == parity])
            if late:
                drain(got.at[:, 0, pl.ds(0, late)], ac_s.at[1])

    if last > 0:
        drain(full.at[0, pl.ds(0, seqs - 1), pl.ds(0, last)], yg_s)
    drain(toks.at[0, pl.ds(0, rows // 2)], tok_s)
    drain(toks.at[0, pl.ds(0, rows // 2)], core_s)
    drain(tots.at[pl.ds(0, n_a - 1)], tot_s)
    yld.wait_send()
    drain(w.at[:, pl.ds(0, depth)], yw_s)
    drain(w.at[:, pl.ds(0, 2 * (n_a - 1) * depth), lanes(0)], x_s)
    for k in range(n_a):
        @pl.when(a == k)
        def _():
            if k < n_a - 1:
                drain(w.at[:, pl.ds(0, 2 * (k + 1) * depth), lanes(0)], z_s.at[1])
            if k > 0:
                drain(w.at[:, pl.ds(0, 2 * (n_a - k) * depth), lanes(0)], z_s.at[0])

    drain(staged, out_sem)
    read_out.wait()


def store(state, read, out, read_out, sem):
    copies = [pltpu.make_async_copy(state, out, sem.at[0]), pltpu.make_async_copy(read, read_out, sem.at[1])]
    for c in copies:
        c.start()
    for c in copies:
        c.wait()


def prompt_states(token_rows, key_weight, value_weight, decays, cos, sin, step, seqs, span, heads, n_sp):
    rows, width = token_rows.shape
    depth, whole = key_weight.shape
    cols = whole // 2
    n_c = cols // 128
    last = n_c - 1
    n_a = n_sp // 2
    hs = heads * seqs
    state_rows = seqs * HEAD_DIM
    dma = pltpu.SemaphoreType.DMA
    bf16 = jnp.bfloat16
    hbm = pl.BlockSpec(memory_space=pl.ANY)
    operands = (token_rows, key_weight, value_weight, decays, cos, sin, *step)
    state, read = pl.pallas_call(
        functools.partial(kernel, (n_sp, seqs, span, heads)),
        out_shape=(
            pltpu.VMEM((whole, state_rows), F32),
            pltpu.VMEM((seqs, whole), bf16),
        ),
        in_specs=[hbm] * 11,
        out_specs=(hbm, hbm),
        scratch_shapes=[
            *(pltpu.VMEM(v.shape, v.dtype) for v in step),
            pltpu.VMEM((whole, state_rows), F32),
            pltpu.VMEM((seqs, whole), bf16),
            pltpu.VMEM((2, rows, width), bf16),
            pltpu.VMEM((n_c, n_sp * depth, 256), bf16),
            pltpu.VMEM((2, hs, span), F32),
            pltpu.VMEM((n_a, 8, 128), F32),
            pltpu.VMEM((2, seqs, span, cols), F32),
            pltpu.VMEM((seqs, n_c, HEAD_DIM, 128), F32),
            pltpu.VMEM((seqs, n_c, HEAD_DIM, 128), bf16),
            pltpu.VMEM((n_a, seqs // 2, n_c, HEAD_DIM, 128), bf16),
            pltpu.VMEM((2, seqs, n_c, HEAD_DIM, 128), bf16),
            pltpu.VMEM((2 * span, 128), F32),
            pltpu.VMEM((2 * span, 128), F32),
            pltpu.VMEM((2, 8, 128), F32),
            pltpu.VMEM((state_rows, whole), F32),
            pltpu.VMEM((state_rows, whole), F32),
            pltpu.VMEM((seqs, whole), F32),
            pltpu.VMEM((2 * n_c, 8, 128), F32),
            pltpu.VMEM((2, rows, 256), F32),
            dma((11,)), dma((n_c,)), dma, dma((2, n_c)),
            dma, dma((seqs,)), dma, dma((seqs,)),
            dma((2,)), dma((n_c, n_sp)), dma, dma((last + n_a,)),
            dma, dma, dma, dma((n_a,)), dma((2, n_a)),
            dma((2,)), dma((seqs // 2, n_c)), dma, dma((seqs, n_c)),
            dma, dma((seqs, n_c)), dma((2,)), dma,
        ],
        compiler_params=pltpu.CompilerParams(
            collective_id=0, has_side_effects=True, vmem_limit_bytes=40 * 1024 * 1024
        ),
    )(*[pltpu.with_memory_space_constraint(v, pltpu.HBM) for v in operands])
    return pl.pallas_call(
        store,
        out_shape=(pltpu.HBM(state.shape, state.dtype), pltpu.HBM(read.shape, read.dtype)),
        in_specs=[pl.BlockSpec(memory_space=pltpu.VMEM)] * 2,
        out_specs=(hbm, hbm),
        scratch_shapes=[dma((2,))],
        compiler_params=pltpu.CompilerParams(vmem_limit_bytes=8 * 1024 * 1024),
    )(*[pltpu.with_memory_space_constraint(v, pltpu.VMEM) for v in (state, read)])


def position_tables(length):
    half = HEAD_DIM // 2
    inverse = np.float32(10000.0) ** (-np.arange(half, dtype=np.float32) * np.float32(2.0 / HEAD_DIM))
    angles = np.arange(length + 8, dtype=np.float32)[:, None] * inverse[None, :].astype(np.float32)
    cosine = np.cos(angles.astype(np.float64)) * HEAD_DIM ** -0.5
    sine = np.sin(angles.astype(np.float64)) * HEAD_DIM ** -0.5
    cos = np.concatenate([cosine] * 4, axis=-1).astype(np.float32)
    sin = np.concatenate([-sine, sine] * 2, axis=-1).astype(np.float32)
    return cos, sin


def shards(
    tokens, key_weight, value_weight, log_decay, new_query, new_key, new_value, step_decay, norm_gain
):
    seqs, span, width = tokens.shape
    heads = key_weight.shape[1] // HEAD_DIM
    n_sp = lax.axis_size("sp")
    token_rows = tokens.reshape(seqs * span, width)
    decays = log_decay.reshape(heads * seqs, span)
    cos, sin = position_tables(span * n_sp)
    step = (new_query, new_key, new_value, step_decay.T, norm_gain.reshape(1, -1))
    state, read = prompt_states(
        token_rows, key_weight, value_weight, decays, jnp.asarray(cos), jnp.asarray(sin), step,
        seqs, span, heads, n_sp,
    )
    return (state.T.reshape(seqs * HEAD_DIM, heads, HEAD_DIM), read)


def solution(mesh):
    placed = (
        P("gr", "sp", None),
        P("sp", "tp"),
        P("sp", "tp"),
        P("tp", "gr", "sp"),
        P("gr", "tp"),
        P("gr", "tp"),
        P("gr", "tp"),
        P("tp", "gr"),
        P("tp"),
    )
    return jax.shard_map(
        shards,
        mesh=mesh,
        in_specs=placed,
        out_specs=(P("gr", "tp", None), P("gr", "tp")),
        check_vma=False,
    )
```
